512 devices in a mesh: sp: 64 (over z, y), tp: 8 (over x, core).
Axes of the slice: x: 4, y: 4, z: 16, core: 2. Of those that a mesh axis runs over, the one named last changes fastest.
Arguments:
- hidden: bfloat16 [12288, 2048], P('sp')
- norm_gain: float32 [2048], replicated, may hold values from 0.1 to 1.9
- query_weight: bfloat16 [2048, 1024], P(None, 'tp'), may hold values from -0.125 to 0.125
- key_weight: bfloat16 [2048, 256], replicated, may hold values from -0.125 to 0.125
- value_weight: bfloat16 [2048, 256], replicated, may hold values from -0.125 to 0.125
- head_bias: float32 [16], P('tp'), may hold values from -10 to -3.5
- output_weight: bfloat16 [1024, 2048], P('tp'), may hold values from -0.1875 to 0.1875
Outputs:
- mixed: bfloat16 [12288, 2048], P('sp')
The draws below stay inside these ranges and needn't reach their ends.
All inputs are finite; a program needn't handle non-finite values.
Results may differ from the reference program's by a relative error of at most 0.014.
Values may be sent and summed in bfloat16 or wider, within the bound.
No kernel may reach another device: no remote copies, remote signals or barrier semaphores. Data moves between devices by JAX's collectives and lax.ppermute only.
A program may use at most 64 MiB of HBM per device.

```python
import math
import jax
import jax.numpy as jnp
from jax import lax

D = 2048
HEADS = 16
KV_HEADS = 4
HEAD_DIM = 64
TOK_DEV = 192
TOKENS = 12288


def draw_hidden(key, part):
    noise_key = jax.random.fold_in(key, 11)
    shift_key = jax.random.fold_in(key, 12)
    block_count = TOKENS // TOK_DEV
    offsets = jax.random.normal(shift_key, (block_count, 1, D), jnp.float32) * 0.8
    noise = jax.random.normal(noise_key, (block_count, TOK_DEV, D), jnp.float32)
    full = noise + offsets
    return full.reshape(TOKENS, D).astype(jnp.bfloat16)


def draw_head_bias(key, part):
    order = jax.random.permutation(jax.random.fold_in(key, 21), HEADS)
    values_key = jax.random.fold_in(key, 22)
    quick = order < HEADS // 2
    slow_value = jax.random.uniform(values_key, (HEADS,), jnp.float32, -9.8, -9.0)
    quick_value = jax.random.uniform(jax.random.fold_in(key, 23), (HEADS,), jnp.float32, -4.3, -3.7)
    return jnp.where(quick, quick_value, slow_value)


def block_scale(stream_key, shape, pieces, least, top_value):
    loudness, own = 1.0, jax.random.fold_in(stream_key, 6)
    for position, shards_of in pieces:
        draws = jnp.exp(jax.random.uniform(jax.random.fold_in(own, position), (shards_of,), jnp.float32, least / len(pieces), top_value / len(pieces)))
        loudness = loudness * jnp.repeat(draws, shape[position] // shards_of).reshape([-1 if axis == position else 1 for axis in range(len(shape))])
    return loudness


def scatter_about(own_key, dims, scale, limit, split=(), kind=jnp.bfloat16):
    loudness = block_scale(own_key, dims, split, -0.22, 0.18) if split else 1.0
    entries = jax.random.normal(own_key, dims, jnp.float32) * scale * loudness
    return jnp.minimum(jnp.maximum(entries, -limit), limit).astype(kind)


def setup_inputs(seed: int = 0) -> dict:
    arg_keys = jax.random.split(jax.random.key(seed), 8)
    return {
        "hidden": draw_hidden(jax.random.fold_in(arg_keys[7], 71), 0),
        "norm_gain": jnp.clip(1.0 + 0.18 * jax.random.normal(arg_keys[1], (D,), jnp.float32), 0.1, 1.9),
        "query_weight": scatter_about(arg_keys[2], (D, HEADS * HEAD_DIM), D ** -0.5, 0.125, ((1, 8),)),
        "key_weight": scatter_about(arg_keys[3], (D, KV_HEADS * HEAD_DIM), D ** -0.5, 0.125),
        "value_weight": scatter_about(arg_keys[4], (D, KV_HEADS * HEAD_DIM), D ** -0.5, 0.125),
        "head_bias": draw_head_bias(jax.random.fold_in(arg_keys[7], 71), 0),
        "output_weight": scatter_about(arg_keys[6], (HEADS * HEAD_DIM, D), (HEADS * HEAD_DIM) ** -0.5, 0.1875, ((0, 8),)),
    }


def reference(hidden, norm_gain, query_weight, key_weight, value_weight, head_bias, output_weight):
    group = HEADS // KV_HEADS
    scale = HEAD_DIM ** (-0.5)
    wide = hidden.astype(jnp.float32)
    normed = (wide * lax.rsqrt(lax.optimization_barrier(jnp.mean(wide * wide, axis=-1, keepdims=True)) + 1e-06) * norm_gain).astype(jnp.bfloat16)
    queries = jnp.dot(normed, query_weight, preferred_element_type=jnp.float32).astype(jnp.bfloat16)
    keys = jnp.dot(normed, key_weight, preferred_element_type=jnp.float32).astype(jnp.bfloat16)
    values = jnp.dot(normed, value_weight, preferred_element_type=jnp.float32).astype(jnp.bfloat16)
    key_heads = jnp.repeat(keys.reshape(TOKENS, KV_HEADS, HEAD_DIM), group, axis=1).astype(jnp.float32)
    value_heads = jnp.repeat(values.reshape(TOKENS, KV_HEADS, HEAD_DIM), group, axis=1).astype(jnp.float32)
    qblock = math.gcd(TOKENS, 256)
    blocks = TOKENS // qblock
    query_blocks = queries.reshape(blocks, qblock, HEADS, HEAD_DIM)
    query_pos = jnp.arange(TOKENS, dtype=jnp.int32).reshape(blocks, qblock)
    key_pos = jnp.arange(TOKENS, dtype=jnp.int32)

    def one_block(args):
        qblk, qpos = args
        z = jnp.einsum('qhd,khd->hqk', qblk.astype(jnp.float32), key_heads) * scale
        z = z + head_bias[:, None, None]
        strict = (key_pos[None, :] < qpos[:, None])[None, :, :]
        keep = jnp.where(strict, jax.nn.log_sigmoid(-z), 0.0)
        between = lax.cumsum(keep, axis=2, reverse=True) - keep
        weight = jnp.where(strict, jnp.exp(jax.nn.log_sigmoid(z) + between), 0.0).astype(jnp.bfloat16)
        out = jnp.einsum('hqk,khd->qhd', weight.astype(jnp.float32), value_heads)
        return out.astype(jnp.bfloat16)
    attended = lax.map(one_block, (query_blocks, query_pos)).reshape(TOKENS, HEADS * HEAD_DIM)
    return jnp.dot(attended, output_weight, preferred_element_type=jnp.float32).astype(jnp.bfloat16)
```

```python
import math

import jax
import jax.numpy as jnp
from jax import lax
from jax.experimental import pallas as pl
from jax.experimental.pallas import tpu as pltpu
from jax.sharding import Mesh
from jax.sharding import PartitionSpec as P

HEAD_DIM = 64
TILE = 256
VMEM = pltpu.VMEM
SMEM = pltpu.SMEM
LIMIT = 56 * 1024 * 1024


def project_kernel(half_ref, hidden_ref, gain_ref, wq_ref, wk_ref, wv_ref, q_ref, kv_ref):
    wide = hidden_ref[...].astype(jnp.float32)
    inv = lax.rsqrt(jnp.mean(wide * wide, axis=-1, keepdims=True) + 1e-06)
    normed = (wide * inv * gain_ref[...]).astype(jnp.bfloat16)
    q = jnp.dot(normed, wq_ref[...], preferred_element_type=jnp.float32).astype(jnp.bfloat16)
    q = q * jnp.bfloat16(HEAD_DIM**-0.5)
    for dest in range(q_ref.shape[0]):
        q_ref[dest] = q
    k = jnp.dot(normed, wk_ref[...], preferred_element_type=jnp.float32)
    v = jnp.dot(normed, wv_ref[...], preferred_element_type=jnp.float32)
    upper = half_ref[0] == 1
    lane = lax.broadcasted_iota(jnp.int32, k.shape, 1)
    k_side = jnp.where(upper, pltpu.roll(k, HEAD_DIM, 1), k)
    v_side = jnp.where(upper, v, pltpu.roll(v, HEAD_DIM, 1))
    kv_ref[...] = jnp.where(lane < HEAD_DIM, k_side, v_side).astype(jnp.bfloat16)


def attend_kernel(rel_ref, bias_ref, q_ref, kv_ref, out_ref, qs, acc, carry):
    key_tiles = kv_ref.shape[0] // TILE
    blocks, tok = q_ref.shape[0], q_ref.shape[1]
    tokens = blocks * tok
    row_tiles = tokens // TILE
    rows = 2 * TILE
    lane = lax.broadcasted_iota(jnp.int32, (tok, 2 * HEAD_DIM), 1)
    for b in range(blocks):
        q = q_ref[b].astype(jnp.float32)
        qs[0, b * tok : (b + 1) * tok, :] = jnp.where(lane < HEAD_DIM, q, 0.0).astype(jnp.bfloat16)
        turned = jnp.where(lane < HEAD_DIM, pltpu.roll(q, HEAD_DIM, 1), 0.0)
        qs[1, b * tok : (b + 1) * tok, :] = turned.astype(jnp.bfloat16)
    acc[...] = jnp.zeros_like(acc)
    carry[...] = jnp.zeros_like(carry)
    from_row = lax.broadcasted_iota(jnp.int32, (TILE, TILE), 0)
    to_col = lax.broadcasted_iota(jnp.int32, (TILE, TILE), 1)
    later = (from_row > to_col).astype(jnp.bfloat16)
    rel = rel_ref[0]

    def step(i, k, masked):
        kv = kv_ref[pl.ds(pl.multiple_of(k * TILE, TILE), TILE), :]
        q = jnp.concatenate([qs[h, i * TILE : (i + 1) * TILE, :] for h in range(2)], axis=0)
        raw = lax.dot_general(q, kv, (((1,), (1,)), ((), ())), preferred_element_type=jnp.float32)
        z = jnp.concatenate([raw[:TILE] + bias_ref[0], raw[TILE:] + bias_ref[1]], axis=0)
        soft = jnp.maximum(z, jnp.log(1.0 + jnp.exp(jnp.minimum(z, 80.0))))
        gain = z - soft
        if masked:
            t = lax.broadcasted_iota(jnp.int32, (rows, TILE), 0) & (TILE - 1)
            s = lax.broadcasted_iota(jnp.int32, (rows, TILE), 1)
            soft = jnp.where(s < t, soft, 0.0)
        between = jnp.dot(soft.astype(jnp.bfloat16), later, preferred_element_type=jnp.float32)
        held = carry[i]
        expo = gain - between - jnp.concatenate([held, held], axis=1)
        weight = jnp.exp(expo)
        if masked:
            weight = jnp.where(s < t, weight, 0.0)
        acc[i] += jnp.dot(weight.astype(jnp.bfloat16), kv, preferred_element_type=jnp.float32)
        carry[i] = held + jnp.broadcast_to(between[:, :1] + soft[:, :1], held.shape)

    for i in range(row_tiles):
        spot = rel + i

        @pl.when((spot >= 0) & (spot < key_tiles))
        def _():
            step(i, spot, True)

        whole = jnp.clip(spot, 0, key_tiles)

        @pl.loop(0, whole)
        def _(n):
            step(i, whole - 1 - n, False)

    wide_lane = lax.broadcasted_iota(jnp.int32, (TILE, 2 * HEAD_DIM), 1)
    for i in range(row_tiles):
        part = jnp.where(
            wide_lane < HEAD_DIM, pltpu.roll(acc[i, :TILE], HEAD_DIM, 1), acc[i, TILE:]
        )
        decay = jnp.exp(-jnp.where(wide_lane < HEAD_DIM, carry[i, :TILE], carry[i, TILE:]))
        out_ref[i * TILE : (i + 1) * TILE, : 2 * HEAD_DIM] = part.astype(jnp.bfloat16)
        out_ref[i * TILE : (i + 1) * TILE, 2 * HEAD_DIM :] = decay.astype(jnp.bfloat16)


def project_out_kernel(heads_ref, weight_ref, out_ref, joined):
    @pl.when(pl.program_id(0) == 0)
    def _():
        for t in range(heads_ref.shape[0]):
            joined[:, t * 128 : (t + 1) * 128] = heads_ref[t]

    out_ref[...] = jnp.dot(
        joined[...], weight_ref[...], preferred_element_type=jnp.float32
    ).astype(jnp.bfloat16)


def local(hidden, norm_gain, query_weight, key_weight, value_weight, head_bias, output_weight):
    rows, width = hidden.shape
    zs, ys, xs = lax.axis_size("z"), lax.axis_size("y"), lax.axis_size("x")
    tps = xs * lax.axis_size("c")
    z, y, x = lax.axis_index("z"), lax.axis_index("y"), lax.axis_index("x")
    mine = 2 * HEAD_DIM
    whole_out = lax.all_gather(output_weight, ("x", "c"), axis=0, tiled=True)

    whole = lambda *shape: pl.BlockSpec(shape, lambda i, pick: (0,) * len(shape))
    side = pl.BlockSpec((width, mine), lambda i, pick: (0, pick[1]))
    pick = jnp.stack([x % 2, x // 2]).astype(jnp.int32)
    q_all, kv = pl.pallas_call(
        project_kernel,
        grid_spec=pltpu.PrefetchScalarGridSpec(
            num_scalar_prefetch=1,
            grid=(1,),
            in_specs=[whole(rows, width), whole(1, width), whole(width, mine), side, side],
            out_specs=[whole(ys, rows, mine), whole(rows, mine)],
        ),
        out_shape=[
            jax.ShapeDtypeStruct((ys, rows, mine), jnp.bfloat16),
            jax.ShapeDtypeStruct((rows, mine), jnp.bfloat16),
        ],
        compiler_params=pltpu.CompilerParams(vmem_limit_bytes=LIMIT),
        cost_estimate=pl.CostEstimate(
            flops=2 * rows * width * 3 * mine, bytes_accessed=2 * width * (rows + 3 * mine), transcendentals=0
        ),
        name="project",
    )(pick, hidden, norm_gain[None, :], query_weight, key_weight, value_weight)

    moved = lax.ppermute(
        kv, ("z", "y"), [(blk, (blk % zs) * ys + blk // zs) for blk in range(zs * ys)]
    )
    row_q = lax.all_to_all(q_all, "y", 0, 0, tiled=True)
    quarter = lax.all_gather(moved, "z", axis=0, tiled=True)

    tokens = ys * rows
    row_tiles = tokens // TILE
    rel = (z * row_tiles - y * (zs * rows // TILE)).astype(jnp.int32).reshape(1)
    part = pl.pallas_call(
        attend_kernel,
        in_specs=[
            pl.BlockSpec(memory_space=SMEM),
            pl.BlockSpec(memory_space=SMEM),
            pl.BlockSpec(memory_space=VMEM),
            pl.BlockSpec(memory_space=VMEM),
        ],
        out_specs=pl.BlockSpec(memory_space=VMEM),
        out_shape=jax.ShapeDtypeStruct((tokens, 2 * mine), jnp.bfloat16),
        scratch_shapes=[
            VMEM((2, tokens, mine), jnp.bfloat16),
            VMEM((row_tiles, 2 * TILE, mine), jnp.float32),
            VMEM((row_tiles, 2 * TILE, mine), jnp.float32),
        ],
        compiler_params=pltpu.CompilerParams(vmem_limit_bytes=LIMIT),
        cost_estimate=pl.CostEstimate(flops=10**10, bytes_accessed=2 * 10**6, transcendentals=0),
        name="attend",
    )(rel, head_bias, row_q, quarter)

    parts = lax.all_to_all(part.reshape(ys, rows, 2 * mine), "y", 0, 0, tiled=True)
    parts = parts.astype(jnp.float32)
    total = parts[0, :, :mine]
    for n in range(1, ys):
        total = parts[n, :, :mine] + parts[n, :, mine:] * total
    attended = total.astype(jnp.bfloat16)
    every_head = lax.all_to_all(
        jnp.broadcast_to(attended[None], (tps, rows, mine)), ("x", "c"), 0, 0, tiled=True
    )
    depth, cols = whole_out.shape
    block = 512
    return pl.pallas_call(
        project_out_kernel,
        grid=(cols // block,),
        in_specs=[
            pl.BlockSpec((tps, rows, mine), lambda n: (0, 0, 0)),
            pl.BlockSpec((depth, block), lambda n: (0, n)),
        ],
        out_specs=pl.BlockSpec((rows, block), lambda n: (0, n)),
        out_shape=jax.ShapeDtypeStruct((rows, cols), jnp.bfloat16),
        scratch_shapes=[VMEM((rows, depth), jnp.bfloat16)],
        compiler_params=pltpu.CompilerParams(vmem_limit_bytes=LIMIT),
        cost_estimate=pl.CostEstimate(
            flops=2 * rows * depth * cols, bytes_accessed=2 * depth * cols, transcendentals=0
        ),
        name="project_out",
    )(every_head, whole_out)


def solution(mesh):
    torus = Mesh(mesh.devices.reshape(16, 4, 4, 2), ("z", "y", "x", "c"))
    sp, tp = ("z", "y"), ("x", "c")
    in_specs = (P(sp, None), P(), P(None, tp), P(), P(), P(tp), P(tp, None))
    return jax.shard_map(
        local, mesh=torus, in_specs=in_specs, out_specs=P(sp, None), check_vma=False
    )
```

```python
import jax
import jax.numpy as jnp
from jax import lax
from jax.experimental import pallas as pl
from jax.experimental.pallas import tpu as pltpu
from jax.sharding import Mesh
from jax.sharding import PartitionSpec as P

HEAD_DIM = 64
TILE = 256
VMEM = pltpu.VMEM
SMEM = pltpu.SMEM
LIMIT = 56 * 1024 * 1024


def project_kernel(
    hidden_ref, gain_ref, wq_hbm, wk_hbm, wv_hbm, q_ref, kv_ref, wq_ref, wk_ref, wv_ref, sems
):
    copies = [
        pltpu.make_async_copy(src, dst, sems.at[n])
        for n, (src, dst) in enumerate(((wk_hbm, wk_ref), (wv_hbm, wv_ref), (wq_hbm, wq_ref)))
    ]
    for copy in copies:
        copy.start()
    x = lax.axis_index("x")
    wide = hidden_ref[...].astype(jnp.float32)
    inv = lax.rsqrt(jnp.mean(wide * wide, axis=-1, keepdims=True) + 1e-06)
    normed = (wide * inv * gain_ref[...]).astype(jnp.bfloat16)

    def own(full):
        pair = jnp.where(x >= 2, full[:, 2 * HEAD_DIM :], full[:, : 2 * HEAD_DIM])
        return pair, pltpu.roll(pair, HEAD_DIM, 1)

    copies[0].wait()
    k, k_turned = own(jnp.dot(normed, wk_ref[...], preferred_element_type=jnp.float32))
    copies[1].wait()
    v, v_turned = own(jnp.dot(normed, wv_ref[...], preferred_element_type=jnp.float32))
    upper = x % 2 == 1
    lane = lax.broadcasted_iota(jnp.int32, k.shape, 1)
    k_side = jnp.where(upper, k_turned, k)
    v_side = jnp.where(upper, v, v_turned)
    kv_ref[...] = jnp.where(lane < HEAD_DIM, k_side, v_side).astype(jnp.bfloat16)
    copies[2].wait()
    q = jnp.dot(normed, wq_ref[...], preferred_element_type=jnp.float32).astype(jnp.bfloat16)
    q = q * jnp.bfloat16(HEAD_DIM**-0.5)
    for dest in range(q_ref.shape[0]):
        q_ref[dest] = q


def attend_kernel(rel_ref, bias_ref, q_ref, kv_ref, out_ref, qs, acc, carry):
    key_tiles = kv_ref.shape[0] // TILE
    blocks, tok = q_ref.shape[0], q_ref.shape[1]
    tokens = blocks * tok
    row_tiles = tokens // TILE
    lane = lax.broadcasted_iota(jnp.int32, (tok, 2 * HEAD_DIM), 1)
    for b in range(blocks):
        q = q_ref[b].astype(jnp.float32)
        qs[b * tok : (b + 1) * tok, :] = jnp.where(lane < HEAD_DIM, q, 0.0).astype(jnp.bfloat16)
        turned = jnp.where(lane < HEAD_DIM, pltpu.roll(q, HEAD_DIM, 1), 0.0)
        qs[tokens + b * tok : tokens + (b + 1) * tok, :] = turned.astype(jnp.bfloat16)
    acc[...] = jnp.zeros_like(acc)
    carry[...] = jnp.zeros_like(carry)
    from_row = lax.broadcasted_iota(jnp.int32, (TILE, TILE), 0)
    to_col = lax.broadcasted_iota(jnp.int32, (TILE, TILE), 1)
    later = (from_row > to_col).astype(jnp.bfloat16)
    rel = rel_ref[0]

    def step(k, masked):
        kv = kv_ref[pl.ds(pl.multiple_of(k * TILE, TILE), TILE), :]
        raw = lax.dot_general(
            qs[...], kv, (((1,), (1,)), ((), ())), preferred_element_type=jnp.float32
        )
        z = jnp.concatenate([raw[:tokens] + bias_ref[0], raw[tokens:] + bias_ref[1]], axis=0)
        soft = jnp.maximum(z, jnp.log(1.0 + jnp.exp(jnp.minimum(z, 80.0))))
        gain = z - soft
        if masked:
            t = lax.broadcasted_iota(jnp.int32, (tokens, TILE), 0)
            t = jnp.concatenate([t, t], axis=0)
            s = lax.broadcasted_iota(jnp.int32, (2 * tokens, TILE), 1) + (k - rel) * TILE
            soft = jnp.where(s < t, soft, 0.0)
        between = jnp.dot(soft.astype(jnp.bfloat16), later, preferred_element_type=jnp.float32)
        held = carry[...]
        weight = jnp.exp(gain - between - jnp.concatenate([held, held], axis=1))
        if masked:
            weight = jnp.where(s < t, weight, 0.0)
        acc[...] += jnp.dot(weight.astype(jnp.bfloat16), kv, preferred_element_type=jnp.float32)
        carry[...] = held + jnp.broadcast_to(between[:, :1] + soft[:, :1], held.shape)

    @pl.when((rel >= 0) & (rel < key_tiles))
    def _():
        @pl.loop(0, row_tiles)
        def _(n):
            step(rel + row_tiles - 1 - n, True)

    whole = jnp.clip(rel, 0, key_tiles)

    @pl.loop(0, whole)
    def _(n):
        step(whole - 1 - n, False)

    wide_lane = lax.broadcasted_iota(jnp.int32, (tokens, 2 * HEAD_DIM), 1)
    first, second = slice(0, tokens), slice(tokens, 2 * tokens)
    part = jnp.where(wide_lane < HEAD_DIM, pltpu.roll(acc[first], HEAD_DIM, 1), acc[second])
    decay = jnp.exp(-jnp.where(wide_lane < HEAD_DIM, carry[first], carry[second]))
    out_ref[:, : 2 * HEAD_DIM] = part.astype(jnp.bfloat16)
    out_ref[:, 2 * HEAD_DIM :] = decay.astype(jnp.bfloat16)


def project_out_kernel(heads_ref, own_ref, other_ref, out_ref, joined):
    c = lax.axis_index("c")
    xs, mine = own_ref.shape[0], own_ref.shape[1]
    for side, core in enumerate((c, 1 - c)):
        for x in range(xs):
            col = (side * xs + x) * mine
            joined[:, col : col + mine] = heads_ref[2 * x + core]
    half = xs * mine
    block = 512
    for n in range(out_ref.shape[1] // block):
        cols = slice(n * block, (n + 1) * block)
        total = jnp.dot(
            joined[:, :half], own_ref[:, :, cols].reshape(half, block), preferred_element_type=jnp.float32
        )
        total += jnp.dot(
            joined[:, half:], other_ref[:, :, cols].reshape(half, block), preferred_element_type=jnp.float32
        )
        out_ref[:, cols] = total.astype(jnp.bfloat16)


def local(hidden, norm_gain, query_weight, key_weight, value_weight, head_bias, output_weight):
    rows, width = hidden.shape
    zs, ys, xs = lax.axis_size("z"), lax.axis_size("y"), lax.axis_size("x")
    tps = xs * lax.axis_size("c")
    z, y = lax.axis_index("z"), lax.axis_index("y")
    mine = 2 * HEAD_DIM
    vmem = pl.BlockSpec(memory_space=VMEM)
    smem = pl.BlockSpec(memory_space=SMEM)
    anywhere = pl.BlockSpec(memory_space=pl.ANY)

    kv_cols = key_weight.shape[1]
    q_all, kv = pl.pallas_call(
        project_kernel,
        in_specs=[vmem, vmem, anywhere, anywhere, anywhere],
        out_specs=[vmem, vmem],
        out_shape=[
            jax.ShapeDtypeStruct((ys, rows, mine), jnp.bfloat16),
            jax.ShapeDtypeStruct((rows, mine), jnp.bfloat16),
        ],
        scratch_shapes=[
            VMEM((width, mine), jnp.bfloat16),
            VMEM((width, kv_cols), jnp.bfloat16),
            VMEM((width, kv_cols), jnp.bfloat16),
            pltpu.SemaphoreType.DMA((3,)),
        ],
        compiler_params=pltpu.CompilerParams(vmem_limit_bytes=LIMIT),
        cost_estimate=pl.CostEstimate(
            flops=2 * rows * width * (mine + 2 * kv_cols),
            bytes_accessed=2 * width * (rows + mine + 2 * kv_cols),
            transcendentals=0,
        ),
        name="project",
    )(hidden, norm_gain[None, :], query_weight, key_weight, value_weight)

    moved = lax.ppermute(
        kv, ("z", "y"), [(blk, (blk % zs) * ys + blk // zs) for blk in range(zs * ys)]
    )
    row_q = lax.all_to_all(q_all, "y", 0, 0, tiled=True)
    row_q, moved, output_weight = lax.optimization_barrier((row_q, moved, output_weight))
    own_rows = lax.all_to_all(
        jnp.broadcast_to(output_weight[None], (xs, *output_weight.shape)), "x", 0, 0, tiled=True
    )
    quarter = lax.all_gather(moved, "z", axis=0, tiled=True)
    quarter, own_rows = lax.optimization_barrier((quarter, own_rows))
    other_rows = lax.ppermute(own_rows, "c", [(0, 1), (1, 0)])

    tokens = ys * rows
    rel = (z * (tokens // TILE) - y * (zs * rows // TILE)).astype(jnp.int32).reshape(1)
    part = pl.pallas_call(
        attend_kernel,
        in_specs=[smem, smem, vmem, vmem],
        out_specs=vmem,
        out_shape=jax.ShapeDtypeStruct((tokens, 2 * mine), jnp.bfloat16),
        scratch_shapes=[
            VMEM((2 * tokens, mine), jnp.bfloat16),
            VMEM((2 * tokens, mine), jnp.float32),
            VMEM((2 * tokens, mine), jnp.float32),
        ],
        compiler_params=pltpu.CompilerParams(vmem_limit_bytes=LIMIT),
        cost_estimate=pl.CostEstimate(flops=10**10, bytes_accessed=2 * 10**6, transcendentals=0),
        name="attend",
    )(rel, head_bias, row_q, quarter)

    parts = lax.all_to_all(part.reshape(ys, rows, 2 * mine), "y", 0, 0, tiled=True)
    parts = parts.astype(jnp.float32)
    total = parts[0, :, :mine]
    for n in range(1, ys):
        total = parts[n, :, :mine] + parts[n, :, mine:] * total
    attended = total.astype(jnp.bfloat16)
    every_head = lax.all_to_all(
        jnp.broadcast_to(attended[None], (tps, rows, mine)), ("x", "c"), 0, 0, tiled=True
    )
    cols = output_weight.shape[1]
    return pl.pallas_call(
        project_out_kernel,
        in_specs=[vmem, vmem, vmem],
        out_specs=vmem,
        out_shape=jax.ShapeDtypeStruct((rows, cols), jnp.bfloat16),
        scratch_shapes=[VMEM((rows, tps * mine), jnp.bfloat16)],
        compiler_params=pltpu.CompilerParams(vmem_limit_bytes=20 * 1024 * 1024),
        cost_estimate=pl.CostEstimate(
            flops=2 * rows * tps * mine * cols, bytes_accessed=2 * tps * mine * cols, transcendentals=0
        ),
        name="project_out",
    )(every_head, own_rows, other_rows)


def solution(mesh):
    torus = Mesh(mesh.devices.reshape(16, 4, 4, 2), ("z", "y", "x", "c"))
    sp, tp = ("z", "y"), ("x", "c")
    in_specs = (P(sp, None), P(), P(None, tp), P(), P(), P(tp), P(tp, None))
    return jax.shard_map(
        local, mesh=torus, in_specs=in_specs, out_specs=P(sp, None), check_vma=False
    )
```

```python
import jax
import jax.numpy as jnp
from jax import lax
from jax.experimental import pallas as pl
from jax.experimental.pallas import tpu as pltpu
from jax.sharding import Mesh
from jax.sharding import PartitionSpec as P

HEAD_DIM = 64
TILE = 256
VMEM = pltpu.VMEM
SMEM = pltpu.SMEM
LIMIT = 56 * 1024 * 1024


def project_kernel(
    hidden_ref, gain_ref, wq_hbm, wk_hbm, wv_hbm, q_ref, kv_ref, wq_ref, wk_ref, wv_ref, sems
):
    copies = [
        pltpu.make_async_copy(src, dst, sems.at[n])
        for n, (src, dst) in enumerate(((wk_hbm, wk_ref), (wv_hbm, wv_ref), (wq_hbm, wq_ref)))
    ]
    for copy in copies:
        copy.start()
    x = lax.axis_index("x")
    wide = hidden_ref[...].astype(jnp.float32)
    inv = lax.rsqrt(jnp.mean(wide * wide, axis=-1, keepdims=True) + 1e-06)
    normed = (wide * inv * gain_ref[...]).astype(jnp.bfloat16)

    def own(full):
        pair = jnp.where(x >= 2, full[:, 2 * HEAD_DIM :], full[:, : 2 * HEAD_DIM])
        return pair, pltpu.roll(pair, HEAD_DIM, 1)

    copies[0].wait()
    k, k_turned = own(jnp.dot(normed, wk_ref[...], preferred_element_type=jnp.float32))
    copies[1].wait()
    v, v_turned = own(jnp.dot(normed, wv_ref[...], preferred_element_type=jnp.float32))
    upper = x % 2 == 1
    lane = lax.broadcasted_iota(jnp.int32, k.shape, 1)
    k_side = jnp.where(upper, k_turned, k)
    v_side = jnp.where(upper, v, v_turned)
    kv = jnp.where(lane < HEAD_DIM, k_side, v_side)
    half = kv_ref.shape[1]
    kv = jnp.where(lax.axis_index("c") == 0, kv[:half], kv[half:]).astype(jnp.bfloat16)
    for dest in range(kv_ref.shape[0]):
        kv_ref[dest] = kv
    copies[2].wait()
    q = jnp.dot(normed, wq_ref[...], preferred_element_type=jnp.float32).astype(jnp.bfloat16)
    q = q * jnp.bfloat16(HEAD_DIM**-0.5)
    q_ref[...] = q


def attend_kernel(bias_ref, q_ref, kv_ref, out_ref, qs, kvs, acc, carry):
    cores, places, half = kv_ref.shape[:3]
    blocks, tok = q_ref.shape[0], q_ref.shape[1]
    mine = 2 * HEAD_DIM
    tokens = blocks * tok
    key_tiles = places * tok // TILE
    a = lax.axis_index("a")
    start = (lax.axis_index("b") * lax.axis_size("y") + lax.axis_index("y")) * tok
    low, high = start // TILE, (start + tok - 1) // TILE
    lane = lax.broadcasted_iota(jnp.int32, (tok, mine), 1)
    for n in range(blocks):
        q = q_ref[n].astype(jnp.float32)
        qs[n * tok : (n + 1) * tok, :] = jnp.where(lane < HEAD_DIM, q, 0.0).astype(jnp.bfloat16)
        turned = jnp.where(lane < HEAD_DIM, pltpu.roll(q, HEAD_DIM, 1), 0.0)
        qs[tokens + n * tok : tokens + (n + 1) * tok, :] = turned.astype(jnp.bfloat16)
    for place in range(places):
        for core in range(cores):
            row = place * tok + core * half
            kvs[row : row + half, :] = kv_ref[core, place]
    acc[...] = jnp.zeros_like(acc)
    carry[...] = jnp.zeros_like(carry)
    from_row = lax.broadcasted_iota(jnp.int32, (TILE, TILE), 0)
    to_col = lax.broadcasted_iota(jnp.int32, (TILE, TILE), 1)
    later = (from_row > to_col).astype(jnp.bfloat16)
    ahead = lax.broadcasted_iota(jnp.int32, (tok, TILE), 1) - lax.broadcasted_iota(
        jnp.int32, (tok, TILE), 0
    )
    shut = jnp.float32(-1e30)

    def step(k, masked):
        kv = kvs[pl.ds(pl.multiple_of(k * TILE, TILE), TILE), :]
        raw = lax.dot_general(
            qs[...], kv, (((1,), (1,)), ((), ())), preferred_element_type=jnp.float32
        )
        groups = []
        for g in range(2 * blocks):
            head, block = divmod(g, blocks)
            closed = (block < a) | ((block == a) & (k > high))
            groups.append(
                raw[g * tok : (g + 1) * tok] + (bias_ref[head] + jnp.where(closed, shut, 0.0))
            )
            if masked:
                limit = jnp.where(block == a, start - k * TILE, 2 * TILE)
                groups[-1] = jnp.where(ahead < limit, groups[-1], shut)
        z = jnp.concatenate(groups, axis=0)
        soft = jnp.maximum(z, jnp.log(1.0 + jnp.exp(jnp.minimum(z, 80.0))))
        gain = z - soft
        between = jnp.dot(soft.astype(jnp.bfloat16), later, preferred_element_type=jnp.float32)
        held = carry[...]
        weight = jnp.exp(gain - between - jnp.concatenate([held, held], axis=1))
        acc[...] += jnp.dot(weight.astype(jnp.bfloat16), kv, preferred_element_type=jnp.float32)
        carry[...] = held + jnp.broadcast_to(between[:, :1] + soft[:, :1], held.shape)

    top = jnp.where(a == blocks - 1, high + 1, key_tiles)

    @pl.loop(0, top)
    def _(n):
        k = top - 1 - n
        edge = (k >= low) & (k <= high)

        @pl.when(edge)
        def _():
            step(k, True)

        @pl.when(jnp.logical_not(edge))
        def _():
            step(k, False)

    mark_row = lax.broadcasted_iota(jnp.int32, (16, mine), 0)
    mark_lane = lax.broadcasted_iota(jnp.int32, (16, mine), 1)
    pick = (mark_row * HEAD_DIM == mark_lane) & (mark_row < 2)
    pick = pick.astype(jnp.bfloat16)
    for n in range(blocks):
        first = slice(n * tok, (n + 1) * tok)
        second = slice(tokens + n * tok, tokens + (n + 1) * tok)
        part = jnp.where(lane < HEAD_DIM, pltpu.roll(acc[first], HEAD_DIM, 1), acc[second])
        decay = jnp.exp(-jnp.where(lane < HEAD_DIM, carry[first], carry[second]))
        out_ref[n, :tok, :] = part.astype(jnp.bfloat16)
        turned = lax.dot_general(
            pick, decay.astype(jnp.bfloat16), (((1,), (1,)), ((), ())), preferred_element_type=jnp.float32
        ).astype(jnp.bfloat16)
        out_ref[n, tok : tok + 16, :] = turned[:, :mine]
        out_ref[n, tok + 16 :, :] = jnp.zeros((16, mine), jnp.bfloat16)
        out_ref[n, tok + 16 :, : tok - mine] = turned[:, mine:]


def combine_kernel(part_ref, out_ref):
    tok, mine = out_ref.shape[1], out_ref.shape[2]
    row = lax.broadcasted_iota(jnp.int32, (16, mine), 0)
    lane = lax.broadcasted_iota(jnp.int32, (16, mine), 1)
    spread = (row == lane // HEAD_DIM).astype(jnp.bfloat16)

    def column(turned):
        return lax.dot_general(
            turned, spread, (((0,), (0,)), ((), ())), preferred_element_type=jnp.float32
        )

    total = part_ref[0, :tok].astype(jnp.float32)
    for n in range(1, part_ref.shape[0]):
        decay = jnp.concatenate(
            [
                column(part_ref[n, tok : tok + 16, :]),
                column(part_ref[n, tok + 16 :, :])[: tok - mine],
            ],
            axis=0,
        )
        total = part_ref[n, :tok].astype(jnp.float32) + decay * total
    attended = total.astype(jnp.bfloat16)
    for dest in range(out_ref.shape[0]):
        out_ref[dest] = attended


def project_out_kernel(heads_ref, own_ref, other_ref, out_ref, joined):
    c = lax.axis_index("c")
    xs, mine = own_ref.shape[0], own_ref.shape[1]
    for side, core in enumerate((c, 1 - c)):
        for x in range(xs):
            col = (side * xs + x) * mine
            joined[:, col : col + mine] = heads_ref[2 * x + core]
    half = xs * mine
    block = 512
    for n in range(out_ref.shape[1] // block):
        cols = slice(n * block, (n + 1) * block)
        total = jnp.dot(
            joined[:, :half], own_ref[:, :, cols].reshape(half, block), preferred_element_type=jnp.float32
        )
        total += jnp.dot(
            joined[:, half:], other_ref[:, :, cols].reshape(half, block), preferred_element_type=jnp.float32
        )
        out_ref[:, cols] = total.astype(jnp.bfloat16)


def local(hidden, norm_gain, query_weight, key_weight, value_weight, head_bias, output_weight):
    rows, width = hidden.shape
    supers, xs = lax.axis_size("a"), lax.axis_size("x")
    places, cores = lax.axis_size("b") * lax.axis_size("y"), lax.axis_size("c")
    tps = xs * cores
    mine = 2 * HEAD_DIM
    vmem = pl.BlockSpec(memory_space=VMEM)
    smem = pl.BlockSpec(memory_space=SMEM)
    anywhere = pl.BlockSpec(memory_space=pl.ANY)

    kv_cols = key_weight.shape[1]
    queries, kv = pl.pallas_call(
        project_kernel,
        in_specs=[vmem, vmem, anywhere, anywhere, anywhere],
        out_specs=[vmem, vmem],
        out_shape=[
            jax.ShapeDtypeStruct((rows, mine), jnp.bfloat16),
            jax.ShapeDtypeStruct((places, rows // cores, mine), jnp.bfloat16),
        ],
        scratch_shapes=[
            VMEM((width, mine), jnp.bfloat16),
            VMEM((width, kv_cols), jnp.bfloat16),
            VMEM((width, kv_cols), jnp.bfloat16),
            pltpu.SemaphoreType.DMA((3,)),
        ],
        compiler_params=pltpu.CompilerParams(vmem_limit_bytes=LIMIT),
        cost_estimate=pl.CostEstimate(
            flops=2 * rows * width * (mine + 2 * kv_cols),
            bytes_accessed=2 * width * (rows + mine + 2 * kv_cols),
            transcendentals=0,
        ),
        name="project",
    )(hidden, norm_gain[None, :], query_weight, key_weight, value_weight)

    kv_half = lax.all_to_all(kv, ("b", "y"), 0, 0, tiled=True)
    kv_half, queries, output_weight = lax.optimization_barrier((kv_half, queries, output_weight))
    own_rows = lax.all_to_all(
        jnp.broadcast_to(output_weight[None], (xs, *output_weight.shape)), "x", 0, 0, tiled=True
    )
    key_value = lax.all_gather(kv_half, "c", axis=0)
    every_q = lax.all_gather(queries, "a", axis=0)
    every_q, key_value, own_rows = lax.optimization_barrier((every_q, key_value, own_rows))
    other_rows = lax.ppermute(own_rows, "c", [(0, 1), (1, 0)])

    tokens = supers * rows
    part = pl.pallas_call(
        attend_kernel,
        in_specs=[smem, vmem, vmem],
        out_specs=vmem,
        out_shape=jax.ShapeDtypeStruct((supers, rows + 32, mine), jnp.bfloat16),
        scratch_shapes=[
            VMEM((2 * tokens, mine), jnp.bfloat16),
            VMEM((places * rows, mine), jnp.bfloat16),
            VMEM((2 * tokens, mine), jnp.float32),
            VMEM((2 * tokens, mine), jnp.float32),
        ],
        compiler_params=pltpu.CompilerParams(vmem_limit_bytes=LIMIT),
        cost_estimate=pl.CostEstimate(flops=10**10, bytes_accessed=2 * 10**6, transcendentals=0),
        name="attend",
    )(head_bias, every_q, key_value)

    parts = lax.all_to_all(part, "a", 0, 0, tiled=True)
    attended = pl.pallas_call(
        combine_kernel,
        in_specs=[vmem],
        out_specs=vmem,
        out_shape=jax.ShapeDtypeStruct((tps, rows, mine), jnp.bfloat16),
        compiler_params=pltpu.CompilerParams(vmem_limit_bytes=16 * 1024 * 1024),
        name="combine",
    )(parts)
    every_head = lax.all_to_all(attended, ("x", "c"), 0, 0, tiled=True)
    cols = output_weight.shape[1]
    return pl.pallas_call(
        project_out_kernel,
        in_specs=[vmem, vmem, vmem],
        out_specs=vmem,
        out_shape=jax.ShapeDtypeStruct((rows, cols), jnp.bfloat16),
        scratch_shapes=[VMEM((rows, tps * mine), jnp.bfloat16)],
        compiler_params=pltpu.CompilerParams(vmem_limit_bytes=20 * 1024 * 1024),
        cost_estimate=pl.CostEstimate(
            flops=2 * rows * tps * mine * cols, bytes_accessed=2 * tps * mine * cols, transcendentals=0
        ),
        name="project_out",
    )(every_head, own_rows, other_rows)


def solution(mesh):
    torus = Mesh(mesh.devices.reshape(4, 4, 4, 4, 2), ("a", "b", "y", "x", "c"))
    sp, tp = ("a", "b", "y"), ("x", "c")
    in_specs = (P(sp, None), P(), P(None, tp), P(), P(), P(tp), P(tp, None))
    return jax.shard_map(
        local, mesh=torus, in_specs=in_specs, out_specs=P(sp, None), check_vma=False
    )
```

```python
import jax
import jax.numpy as jnp
from jax import lax
from jax.experimental import pallas as pl
from jax.experimental.pallas import tpu as pltpu
from jax.sharding import Mesh
from jax.sharding import PartitionSpec as P

HEAD_DIM = 64
TILE = 256
VMEM = pltpu.VMEM
SMEM = pltpu.SMEM
LIMIT = 56 * 1024 * 1024


def project_kernel(
    hidden_ref, gain_ref, wq_hbm, wk_hbm, wv_hbm, q_ref, kv_ref, wq_ref, wk_ref, wv_ref, normed_ref, sems
):
    copies = [
        pltpu.make_async_copy(src, dst, sems.at[n])
        for n, (src, dst) in enumerate(((wk_hbm, wk_ref), (wv_hbm, wv_ref), (wq_hbm, wq_ref)))
    ]
    for copy in copies:
        copy.start()
    x = lax.axis_index("x")
    piece = 32
    for row in range(0, hidden_ref.shape[0], piece):
        wide = hidden_ref[row : row + piece, :].astype(jnp.float32)
        inv = lax.rsqrt(jnp.mean(wide * wide, axis=-1, keepdims=True) + 1e-06)
        normed_ref[row : row + piece, :] = (wide * inv * gain_ref[...]).astype(jnp.bfloat16)
    normed = normed_ref[...]

    def own(full):
        pair = jnp.where(x >= 2, full[:, 2 * HEAD_DIM :], full[:, : 2 * HEAD_DIM])
        return pair, pltpu.roll(pair, HEAD_DIM, 1)

    copies[0].wait()
    k, k_turned = own(jnp.dot(normed, wk_ref[...], preferred_element_type=jnp.float32))
    copies[1].wait()
    v, v_turned = own(jnp.dot(normed, wv_ref[...], preferred_element_type=jnp.float32))
    upper = x % 2 == 1
    lane = lax.broadcasted_iota(jnp.int32, k.shape, 1)
    k_side = jnp.where(upper, k_turned, k)
    v_side = jnp.where(upper, v, v_turned)
    kv = jnp.where(lane < HEAD_DIM, k_side, v_side)
    half = kv_ref.shape[0]
    kv = jnp.where(lax.axis_index("c") == 0, kv[:half], kv[half:]).astype(jnp.bfloat16)
    kv_ref[...] = kv
    copies[2].wait()
    q = jnp.dot(normed, wq_ref[...], preferred_element_type=jnp.float32).astype(jnp.bfloat16)
    q = q * jnp.bfloat16(HEAD_DIM**-0.5)
    for dest in range(q_ref.shape[0]):
        q_ref[dest] = q


def attend_kernel(bias_ref, q_ref, kv_ref, out_ref, qs, kvs, acc, carry):
    cores, places, half = kv_ref.shape[:3]
    blocks, tok = q_ref.shape[0], q_ref.shape[1]
    mine = 2 * HEAD_DIM
    key_tiles = places * tok // TILE
    tokens = blocks * tok
    row_tiles = tokens // TILE
    lane = lax.broadcasted_iota(jnp.int32, (tok, 2 * HEAD_DIM), 1)
    for b in range(blocks):
        q = q_ref[b].astype(jnp.float32)
        qs[b * tok : (b + 1) * tok, :] = jnp.where(lane < HEAD_DIM, q, 0.0).astype(jnp.bfloat16)
        turned = jnp.where(lane < HEAD_DIM, pltpu.roll(q, HEAD_DIM, 1), 0.0)
        qs[tokens + b * tok : tokens + (b + 1) * tok, :] = turned.astype(jnp.bfloat16)
    for place in range(places):
        for core in range(cores):
            row = place * tok + core * half
            kvs[row : row + half, :] = kv_ref[core, place]
    acc[...] = jnp.zeros_like(acc)
    carry[...] = jnp.zeros_like(carry)
    from_row = lax.broadcasted_iota(jnp.int32, (TILE, TILE), 0)
    to_col = lax.broadcasted_iota(jnp.int32, (TILE, TILE), 1)
    later = (from_row > to_col).astype(jnp.bfloat16)
    rel = lax.axis_index("z") * row_tiles - lax.axis_index("y") * key_tiles

    def step(k, masked):
        kv = kvs[pl.ds(pl.multiple_of(k * TILE, TILE), TILE), :]
        raw = lax.dot_general(
            qs[...], kv, (((1,), (1,)), ((), ())), preferred_element_type=jnp.float32
        )
        z = jnp.concatenate([raw[:tokens] + bias_ref[0], raw[tokens:] + bias_ref[1]], axis=0)
        soft = jnp.maximum(z, jnp.log(1.0 + jnp.exp(jnp.minimum(z, 80.0))))
        gain = z - soft
        if masked:
            t = lax.broadcasted_iota(jnp.int32, (tokens, TILE), 0)
            t = jnp.concatenate([t, t], axis=0)
            s = lax.broadcasted_iota(jnp.int32, (2 * tokens, TILE), 1) + (k - rel) * TILE
            soft = jnp.where(s < t, soft, 0.0)
        between = jnp.dot(soft.astype(jnp.bfloat16), later, preferred_element_type=jnp.float32)
        held = carry[...]
        weight = jnp.exp(gain - between - jnp.concatenate([held, held], axis=1))
        if masked:
            weight = jnp.where(s < t, weight, 0.0)
        acc[...] += jnp.dot(weight.astype(jnp.bfloat16), kv, preferred_element_type=jnp.float32)
        carry[...] = held + jnp.broadcast_to(between[:, :1] + soft[:, :1], held.shape)

    @pl.when((rel >= 0) & (rel < key_tiles))
    def _():
        @pl.loop(0, row_tiles)
        def _(n):
            step(rel + row_tiles - 1 - n, True)

    whole = jnp.clip(rel, 0, key_tiles)

    @pl.loop(0, whole)
    def _(n):
        step(whole - 1 - n, False)

    mark_row = lax.broadcasted_iota(jnp.int32, (16, mine), 0)
    mark_lane = lax.broadcasted_iota(jnp.int32, (16, mine), 1)
    pick = (mark_row * HEAD_DIM == mark_lane) & (mark_row < 2)
    pick = pick.astype(jnp.bfloat16)
    for n in range(blocks):
        first = slice(n * tok, (n + 1) * tok)
        second = slice(tokens + n * tok, tokens + (n + 1) * tok)
        part = jnp.where(lane < HEAD_DIM, pltpu.roll(acc[first], HEAD_DIM, 1), acc[second])
        decay = jnp.exp(-jnp.where(lane < HEAD_DIM, carry[first], carry[second]))
        out_ref[n, :tok, :] = part.astype(jnp.bfloat16)
        turned = lax.dot_general(
            pick, decay.astype(jnp.bfloat16), (((1,), (1,)), ((), ())), preferred_element_type=jnp.float32
        ).astype(jnp.bfloat16)
        out_ref[n, tok : tok + 16, :] = turned[:, :mine]
        out_ref[n, tok + 16 :, :] = jnp.zeros((16, mine), jnp.bfloat16)
        out_ref[n, tok + 16 :, : tok - mine] = turned[:, mine:]


def combine_kernel(part_ref, out_ref):
    tok, mine = out_ref.shape[1], out_ref.shape[2]
    row = lax.broadcasted_iota(jnp.int32, (16, mine), 0)
    lane = lax.broadcasted_iota(jnp.int32, (16, mine), 1)
    spread = (row == lane // HEAD_DIM).astype(jnp.bfloat16)

    def column(turned):
        return lax.dot_general(
            turned, spread, (((0,), (0,)), ((), ())), preferred_element_type=jnp.float32
        )

    total = part_ref[0, :tok].astype(jnp.float32)
    for n in range(1, part_ref.shape[0]):
        decay = jnp.concatenate(
            [
                column(part_ref[n, tok : tok + 16, :]),
                column(part_ref[n, tok + 16 :, :])[: tok - mine],
            ],
            axis=0,
        )
        total = part_ref[n, :tok].astype(jnp.float32) + decay * total
    attended = total.astype(jnp.bfloat16)
    for dest in range(out_ref.shape[0]):
        out_ref[dest] = attended


def project_out_kernel(heads_ref, own_ref, other_ref, out_ref, joined):
    c = lax.axis_index("c")
    xs, mine = own_ref.shape[0], own_ref.shape[1]
    for side, core in enumerate((c, 1 - c)):
        for x in range(xs):
            col = (side * xs + x) * mine
            joined[:, col : col + mine] = heads_ref[2 * x + core]
    half = xs * mine
    block = 512
    for n in range(out_ref.shape[1] // block):
        cols = slice(n * block, (n + 1) * block)
        total = jnp.dot(
            joined[:, :half], own_ref[:, :, cols].reshape(half, block), preferred_element_type=jnp.float32
        )
        total += jnp.dot(
            joined[:, half:], other_ref[:, :, cols].reshape(half, block), preferred_element_type=jnp.float32
        )
        out_ref[:, cols] = total.astype(jnp.bfloat16)


def local(hidden, norm_gain, query_weight, key_weight, value_weight, head_bias, output_weight):
    rows, width = hidden.shape
    zs, ys, xs = lax.axis_size("z"), lax.axis_size("y"), lax.axis_size("x")
    cores = lax.axis_size("c")
    tps = xs * cores
    mine = 2 * HEAD_DIM
    vmem = pl.BlockSpec(memory_space=VMEM)
    smem = pl.BlockSpec(memory_space=SMEM)
    anywhere = pl.BlockSpec(memory_space=pl.ANY)

    kv_cols = key_weight.shape[1]
    queries, kv = pl.pallas_call(
        project_kernel,
        in_specs=[vmem, vmem, anywhere, anywhere, anywhere],
        out_specs=[vmem, vmem],
        out_shape=[
            jax.ShapeDtypeStruct((ys, rows, mine), jnp.bfloat16),
            jax.ShapeDtypeStruct((rows // cores, mine), jnp.bfloat16),
        ],
        scratch_shapes=[
            VMEM((width, mine), jnp.bfloat16),
            VMEM((width, kv_cols), jnp.bfloat16),
            VMEM((width, kv_cols), jnp.bfloat16),
            VMEM((rows, width), jnp.bfloat16),
            pltpu.SemaphoreType.DMA((3,)),
        ],
        compiler_params=pltpu.CompilerParams(vmem_limit_bytes=LIMIT),
        cost_estimate=pl.CostEstimate(
            flops=2 * rows * width * (mine + 2 * kv_cols),
            bytes_accessed=2 * width * (rows + mine + 2 * kv_cols),
            transcendentals=0,
        ),
        name="project",
    )(hidden, norm_gain[None, :], query_weight, key_weight, value_weight)

    moved = lax.ppermute(
        kv, ("z", "y"), [(blk, (blk % zs) * ys + blk // zs) for blk in range(zs * ys)]
    )
    row_q = lax.all_to_all(queries, "y", 0, 0, tiled=True)
    row_q, moved, output_weight = lax.optimization_barrier((row_q, moved, output_weight))
    own_rows = lax.all_to_all(
        jnp.broadcast_to(output_weight[None], (xs, *output_weight.shape)), "x", 0, 0, tiled=True
    )
    quarter_half = lax.all_gather(moved, "z", axis=0)
    quarter = lax.all_gather(quarter_half, "c", axis=0)
    quarter, own_rows = lax.optimization_barrier((quarter, own_rows))
    other_rows = lax.ppermute(own_rows, "c", [(0, 1), (1, 0)])

    tokens = ys * rows
    part = pl.pallas_call(
        attend_kernel,
        in_specs=[smem, vmem, vmem],
        out_specs=vmem,
        out_shape=jax.ShapeDtypeStruct((ys, rows + 32, mine), jnp.bfloat16),
        scratch_shapes=[
            VMEM((2 * tokens, mine), jnp.bfloat16),
            VMEM((zs * rows, mine), jnp.bfloat16),
            VMEM((2 * tokens, mine), jnp.float32),
            VMEM((2 * tokens, mine), jnp.float32),
        ],
        compiler_params=pltpu.CompilerParams(vmem_limit_bytes=LIMIT),
        cost_estimate=pl.CostEstimate(flops=10**10, bytes_accessed=2 * 10**6, transcendentals=0),
        name="attend",
    )(head_bias, row_q, quarter)

    parts = lax.all_to_all(part, "y", 0, 0, tiled=True)
    attended = pl.pallas_call(
        combine_kernel,
        in_specs=[vmem],
        out_specs=vmem,
        out_shape=jax.ShapeDtypeStruct((tps, rows, mine), jnp.bfloat16),
        compiler_params=pltpu.CompilerParams(vmem_limit_bytes=16 * 1024 * 1024),
        name="combine",
    )(parts)
    every_head = lax.all_to_all(attended, ("x", "c"), 0, 0, tiled=True)
    cols = output_weight.shape[1]
    return pl.pallas_call(
        project_out_kernel,
        in_specs=[vmem, vmem, vmem],
        out_specs=vmem,
        out_shape=jax.ShapeDtypeStruct((rows, cols), jnp.bfloat16),
        scratch_shapes=[VMEM((rows, tps * mine), jnp.bfloat16)],
        compiler_params=pltpu.CompilerParams(vmem_limit_bytes=20 * 1024 * 1024),
        cost_estimate=pl.CostEstimate(
            flops=2 * rows * tps * mine * cols, bytes_accessed=2 * tps * mine * cols, transcendentals=0
        ),
        name="project_out",
    )(every_head, own_rows, other_rows)


def solution(mesh):
    torus = Mesh(mesh.devices.reshape(16, 4, 4, 2), ("z", "y", "x", "c"))
    sp, tp = ("z", "y"), ("x", "c")
    in_specs = (P(sp, None), P(), P(None, tp), P(), P(), P(tp), P(tp, None))
    return jax.shard_map(
        local, mesh=torus, in_specs=in_specs, out_specs=P(sp, None), check_vma=False
    )
```

```python
import jax
import jax.numpy as jnp
from jax import lax
from jax.experimental import pallas as pl
from jax.experimental.pallas import tpu as pltpu
from jax.sharding import Mesh
from jax.sharding import PartitionSpec as P


HEAD_DIM = 64
TILE = 256
VMEM = pltpu.VMEM
SMEM = pltpu.SMEM
LIMIT = 56 * 1024 * 1024


PIECES = 4
ROWS_AT_ONCE = 32
NEAR = ((-6, -5, -3, -4), (-2, -1, 1, 0), (5, 4, 2, 3), (9, 8, 6, 7))


def project_kernel(
    hidden_hbm, gain_ref, wq_hbm, wk_hbm, wv_hbm, q_ref, kv_ref, hidden_ref, wq_ref, wkv_ref, normed_ref, sems
):
    rows, width = hidden_ref.shape
    mine = 2 * HEAD_DIM
    depth = width // PIECES
    x = lax.axis_index("x")
    cols = pl.ds(pl.multiple_of((x // 2) * mine, mine), mine)
    pieces = rows // ROWS_AT_ONCE
    copies = []
    for n in range(pieces):
        part = slice(n * ROWS_AT_ONCE, (n + 1) * ROWS_AT_ONCE)
        copies.append(
            pltpu.make_async_copy(hidden_hbm.at[part, :], hidden_ref.at[part, :], sems.at[n])
        )
    for n in range(PIECES):
        part = slice(n * depth, (n + 1) * depth)
        for side, src in enumerate((wk_hbm, wv_hbm)):
            copies.append(
                pltpu.make_async_copy(
                    src.at[part, cols],
                    wkv_ref.at[part, side * mine : (side + 1) * mine],
                    sems.at[pieces + 2 * n + side],
                )
            )
    for n in range(PIECES):
        part = slice(n * depth, (n + 1) * depth)
        copies.append(
            pltpu.make_async_copy(
                wq_hbm.at[part, :], wq_ref.at[part, :], sems.at[pieces + 2 * PIECES + n]
            )
        )
    for copy in copies:
        copy.start()
    for n in range(pieces):
        part = slice(n * ROWS_AT_ONCE, (n + 1) * ROWS_AT_ONCE)
        copies[n].wait()
        wide = hidden_ref[part, :].astype(jnp.float32)
        inv = lax.rsqrt(jnp.mean(wide * wide, axis=-1, keepdims=True) + 1e-06)
        normed_ref[part, :] = (wide * inv * gain_ref[...]).astype(jnp.bfloat16)

    both = jnp.zeros((rows, 2 * mine), jnp.float32)
    for n in range(PIECES):
        part = slice(n * depth, (n + 1) * depth)
        copies[pieces + 2 * n].wait()
        copies[pieces + 2 * n + 1].wait()
        both += jnp.dot(normed_ref[:, part], wkv_ref[part, :], preferred_element_type=jnp.float32)
    k, v = both[:, :mine], both[:, mine:]
    upper = x % 2 == 1
    lane = lax.broadcasted_iota(jnp.int32, k.shape, 1)
    k_side = jnp.where(upper, pltpu.roll(k, HEAD_DIM, 1), k)
    v_side = jnp.where(upper, v, pltpu.roll(v, HEAD_DIM, 1))
    kv = jnp.where(lane < HEAD_DIM, k_side, v_side)
    half = kv_ref.shape[0]
    kv_ref[...] = jnp.where(lax.axis_index("c") == 0, kv[:half], kv[half:]).astype(jnp.bfloat16)

    q = jnp.zeros((rows, mine), jnp.float32)
    for n in range(PIECES):
        part = slice(n * depth, (n + 1) * depth)
        copies[pieces + 2 * PIECES + n].wait()
        q += jnp.dot(normed_ref[:, part], wq_ref[part, :], preferred_element_type=jnp.float32)
    q = q.astype(jnp.bfloat16) * jnp.bfloat16(HEAD_DIM**-0.5)
    for dest in range(q_ref.shape[0]):
        q_ref[dest] = q


def attend_kernel(bias_ref, q_ref, kv_ref, out_ref, qs, kvs, acc, carry):
    cores, places, half = kv_ref.shape[:3]
    blocks, tok = q_ref.shape[0], q_ref.shape[1]
    mine = 2 * HEAD_DIM
    key_tiles = places * tok // TILE
    tokens = blocks * tok
    row_tiles = tokens // TILE
    lane = lax.broadcasted_iota(jnp.int32, (tok, 2 * HEAD_DIM), 1)
    for b in range(blocks):
        q = q_ref[b].astype(jnp.float32)
        qs[b * tok : (b + 1) * tok, :] = jnp.where(lane < HEAD_DIM, q, 0.0).astype(jnp.bfloat16)
        turned = jnp.where(lane < HEAD_DIM, pltpu.roll(q, HEAD_DIM, 1), 0.0)
        qs[tokens + b * tok : tokens + (b + 1) * tok, :] = turned.astype(jnp.bfloat16)
    own = lax.axis_index("y")
    span = len(NEAR)
    for row in range(span):
        for turn in range(span):
            source = lax.rem(span * own + NEAR[row][turn] + places, places)
            place = row * span + lax.rem(own + turn, span)
            for core in range(cores):
                at = pl.multiple_of(place * tok + core * half, 32)
                kvs[pl.ds(at, half), :] = kv_ref[core, source]
    acc[...] = jnp.zeros_like(acc)
    carry[...] = jnp.zeros_like(carry)
    from_row = lax.broadcasted_iota(jnp.int32, (TILE, TILE), 0)
    to_col = lax.broadcasted_iota(jnp.int32, (TILE, TILE), 1)
    later = (from_row > to_col).astype(jnp.bfloat16)
    rel = lax.axis_index("z") * row_tiles - own * key_tiles

    def step(k, masked):
        kv = kvs[pl.ds(pl.multiple_of(k * TILE, TILE), TILE), :]
        raw = lax.dot_general(
            qs[...], kv, (((1,), (1,)), ((), ())), preferred_element_type=jnp.float32
        )
        z = jnp.concatenate([raw[:tokens] + bias_ref[0], raw[tokens:] + bias_ref[1]], axis=0)
        soft = jnp.maximum(z, jnp.log(1.0 + jnp.exp(jnp.minimum(z, 80.0))))
        gain = z - soft
        if masked:
            t = lax.broadcasted_iota(jnp.int32, (tokens, TILE), 0)
            t = jnp.concatenate([t, t], axis=0)
            s = lax.broadcasted_iota(jnp.int32, (2 * tokens, TILE), 1) + (k - rel) * TILE
            soft = jnp.where(s < t, soft, 0.0)
        between = jnp.dot(soft.astype(jnp.bfloat16), later, preferred_element_type=jnp.float32)
        held = carry[...]
        weight = jnp.exp(gain - between - jnp.concatenate([held, held], axis=1))
        if masked:
            weight = jnp.where(s < t, weight, 0.0)
        acc[...] += jnp.dot(weight.astype(jnp.bfloat16), kv, preferred_element_type=jnp.float32)
        carry[...] = held + jnp.broadcast_to(between[:, :1] + soft[:, :1], held.shape)

    @pl.when((rel >= 0) & (rel < key_tiles))
    def _():
        @pl.loop(0, row_tiles)
        def _(n):
            step(rel + row_tiles - 1 - n, True)

    whole = jnp.clip(rel, 0, key_tiles)

    @pl.loop(0, whole)
    def _(n):
        step(whole - 1 - n, False)

    mark_row = lax.broadcasted_iota(jnp.int32, (16, mine), 0)
    mark_lane = lax.broadcasted_iota(jnp.int32, (16, mine), 1)
    pick = (mark_row * HEAD_DIM == mark_lane) & (mark_row < 2)
    pick = pick.astype(jnp.bfloat16)
    for n in range(blocks):
        first = slice(n * tok, (n + 1) * tok)
        second = slice(tokens + n * tok, tokens + (n + 1) * tok)
        part = jnp.where(lane < HEAD_DIM, pltpu.roll(acc[first], HEAD_DIM, 1), acc[second])
        decay = jnp.exp(-jnp.where(lane < HEAD_DIM, carry[first], carry[second]))
        out_ref[n, :tok, :] = part.astype(jnp.bfloat16)
        turned = lax.dot_general(
            pick, decay.astype(jnp.bfloat16), (((1,), (1,)), ((), ())), preferred_element_type=jnp.float32
        ).astype(jnp.bfloat16)
        out_ref[n, tok : tok + 16, :] = turned[:, :mine]
        out_ref[n, tok + 16 :, :] = jnp.zeros((16, mine), jnp.bfloat16)
        out_ref[n, tok + 16 :, : tok - mine] = turned[:, mine:]


def combine_kernel(part_ref, out_ref):
    tok, mine = out_ref.shape[1], out_ref.shape[2]
    row = lax.broadcasted_iota(jnp.int32, (16, mine), 0)
    lane = lax.broadcasted_iota(jnp.int32, (16, mine), 1)
    spread = (row == lane // HEAD_DIM).astype(jnp.bfloat16)

    def column(turned):
        return lax.dot_general(
            turned, spread, (((0,), (0,)), ((), ())), preferred_element_type=jnp.float32
        )

    total = part_ref[0, :tok].astype(jnp.float32)
    for n in range(1, part_ref.shape[0]):
        decay = jnp.concatenate(
            [
                column(part_ref[n, tok : tok + 16, :]),
                column(part_ref[n, tok + 16 :, :])[: tok - mine],
            ],
            axis=0,
        )
        total = part_ref[n, :tok].astype(jnp.float32) + decay * total
    attended = total.astype(jnp.bfloat16)
    for dest in range(out_ref.shape[0]):
        out_ref[dest] = attended


def project_out_kernel(heads_ref, own_ref, other_ref, out_ref, joined):
    c = lax.axis_index("c")
    xs, mine = own_ref.shape[0], own_ref.shape[1]
    for side, core in enumerate((c, 1 - c)):
        for x in range(xs):
            col = (side * xs + x) * mine
            joined[:, col : col + mine] = heads_ref[2 * x + core]
    half = xs * mine
    block = 512
    for n in range(out_ref.shape[1] // block):
        cols = slice(n * block, (n + 1) * block)
        total = jnp.dot(
            joined[:, :half], own_ref[:, :, cols].reshape(half, block), preferred_element_type=jnp.float32
        )
        total += jnp.dot(
            joined[:, half:], other_ref[:, :, cols].reshape(half, block), preferred_element_type=jnp.float32
        )
        out_ref[:, cols] = total.astype(jnp.bfloat16)


def local(hidden, norm_gain, query_weight, key_weight, value_weight, head_bias, output_weight):
    rows, width = hidden.shape
    zs, ys, xs = lax.axis_size("z"), lax.axis_size("y"), lax.axis_size("x")
    cores = lax.axis_size("c")
    tps = xs * cores
    mine = 2 * HEAD_DIM
    vmem = pl.BlockSpec(memory_space=VMEM)
    smem = pl.BlockSpec(memory_space=SMEM)
    anywhere = pl.BlockSpec(memory_space=pl.ANY)

    queries, kv = pl.pallas_call(
        project_kernel,
        in_specs=[anywhere, vmem, anywhere, anywhere, anywhere],
        out_specs=[vmem, vmem],
        out_shape=[
            jax.ShapeDtypeStruct((ys, rows, mine), jnp.bfloat16),
            jax.ShapeDtypeStruct((rows // cores, mine), jnp.bfloat16),
        ],
        scratch_shapes=[
            VMEM((rows, width), jnp.bfloat16),
            VMEM((width, mine), jnp.bfloat16),
            VMEM((width, 2 * mine), jnp.bfloat16),
            VMEM((rows, width), jnp.bfloat16),
            pltpu.SemaphoreType.DMA((rows // ROWS_AT_ONCE + 3 * PIECES,)),
        ],
        compiler_params=pltpu.CompilerParams(vmem_limit_bytes=LIMIT),
        cost_estimate=pl.CostEstimate(
            flops=2 * rows * width * 3 * mine,
            bytes_accessed=2 * width * (rows + 3 * mine),
            transcendentals=0,
        ),
        name="project",
    )(hidden, norm_gain[None, :], query_weight, key_weight, value_weight)

    pairs = []
    for z in range(zs):
        for y in range(ys):
            super_row, row = divmod(z, ys)
            near = (ys * super_row + NEAR[row][(y - super_row) % ys]) % zs
            pairs.append((z * ys + y, near * ys + super_row))
    moved = lax.ppermute(kv, ("z", "y"), pairs)
    row_q = lax.all_to_all(queries, "y", 0, 0, tiled=True)
    fan = jnp.broadcast_to(output_weight[None], (xs, *output_weight.shape))
    row_q, moved, fan = lax.optimization_barrier((row_q, moved, fan))
    own_rows = lax.all_to_all(fan, "x", 0, 0, tiled=True)
    quarter_half = lax.all_gather(moved, "z", axis=0)
    quarter = lax.all_gather(quarter_half, "c", axis=0)
    quarter, own_rows = lax.optimization_barrier((quarter, own_rows))
    other_rows = lax.ppermute(own_rows, "c", [(0, 1), (1, 0)])

    tokens = ys * rows
    part = pl.pallas_call(
        attend_kernel,
        in_specs=[smem, vmem, vmem],
        out_specs=vmem,
        out_shape=jax.ShapeDtypeStruct((ys, rows + 32, mine), jnp.bfloat16),
        scratch_shapes=[
            VMEM((2 * tokens, mine), jnp.bfloat16),
            VMEM((zs * rows, mine), jnp.bfloat16),
            VMEM((2 * tokens, mine), jnp.float32),
            VMEM((2 * tokens, mine), jnp.float32),
        ],
        compiler_params=pltpu.CompilerParams(vmem_limit_bytes=LIMIT),
        cost_estimate=pl.CostEstimate(flops=10**10, bytes_accessed=2 * 10**6, transcendentals=0),
        name="attend",
    )(head_bias, row_q, quarter)

    parts = lax.all_to_all(part, "y", 0, 0, tiled=True)
    attended = pl.pallas_call(
        combine_kernel,
        in_specs=[vmem],
        out_specs=vmem,
        out_shape=jax.ShapeDtypeStruct((tps, rows, mine), jnp.bfloat16),
        compiler_params=pltpu.CompilerParams(vmem_limit_bytes=16 * 1024 * 1024),
        name="combine",
    )(parts)
    every_head = lax.all_to_all(attended, ("x", "c"), 0, 0, tiled=True)
    cols = output_weight.shape[1]
    return pl.pallas_call(
        project_out_kernel,
        in_specs=[vmem, vmem, vmem],
        out_specs=vmem,
        out_shape=jax.ShapeDtypeStruct((rows, cols), jnp.bfloat16),
        scratch_shapes=[VMEM((rows, tps * mine), jnp.bfloat16)],
        compiler_params=pltpu.CompilerParams(vmem_limit_bytes=20 * 1024 * 1024),
        cost_estimate=pl.CostEstimate(
            flops=2 * rows * tps * mine * cols, bytes_accessed=2 * tps * mine * cols, transcendentals=0
        ),
        name="project_out",
    )(every_head, own_rows, other_rows)


def solution(mesh):
    torus = Mesh(mesh.devices.reshape(16, 4, 4, 2), ("z", "y", "x", "c"))
    sp, tp = ("z", "y"), ("x", "c")
    in_specs = (P(sp, None), P(), P(None, tp), P(), P(), P(tp), P(tp, None))
    return jax.shard_map(
        local, mesh=torus, in_specs=in_specs, out_specs=P(sp, None), check_vma=False
    )
```

```python
import math

import jax
import jax.numpy as jnp
from jax import lax
from jax.experimental import pallas as pl
from jax.experimental.pallas import tpu as pltpu
from jax.sharding import Mesh
from jax.sharding import PartitionSpec as P


HEAD_DIM = 64
TILE = 256
VMEM = pltpu.VMEM
SMEM = pltpu.SMEM
LIMIT = 56 * 1024 * 1024
HELD = 64 * math.log(2.0)


PIECES = 4
ROWS_AT_ONCE = 32
NEAR = ((-6, -5, -3, -4), (-2, -1, 1, 0), (5, 4, 2, 3), (9, 8, 6, 7))


def project_kernel(
    hidden_hbm, gain_ref, wq_hbm, wk_hbm, wv_hbm, q_ref, kv_ref, hidden_ref, wq_ref, wkv_ref, normed_ref, turn_ref, sems
):
    rows, width = hidden_ref.shape
    mine = 2 * HEAD_DIM
    depth = width // PIECES
    x = lax.axis_index("x")
    cols = pl.ds(pl.multiple_of((x // 2) * mine, mine), mine)
    pieces = rows // ROWS_AT_ONCE
    copies = []
    for n in range(pieces):
        part = slice(n * ROWS_AT_ONCE, (n + 1) * ROWS_AT_ONCE)
        copies.append(
            pltpu.make_async_copy(hidden_hbm.at[part, :], hidden_ref.at[part, :], sems.at[n])
        )
    for n in range(PIECES):
        part = slice(n * depth, (n + 1) * depth)
        for side, src in enumerate((wk_hbm, wv_hbm)):
            copies.append(
                pltpu.make_async_copy(
                    src.at[part, cols],
                    wkv_ref.at[part, side * mine : (side + 1) * mine],
                    sems.at[pieces + 2 * n + side],
                )
            )
    for n in range(PIECES):
        part = slice(n * depth, (n + 1) * depth)
        copies.append(
            pltpu.make_async_copy(
                wq_hbm.at[part, :], wq_ref.at[part, :], sems.at[pieces + 2 * PIECES + n]
            )
        )
    for copy in copies:
        copy.start()
    for n in range(pieces):
        part = slice(n * ROWS_AT_ONCE, (n + 1) * ROWS_AT_ONCE)
        copies[n].wait()
        wide = hidden_ref[part, :].astype(jnp.float32)
        inv = lax.rsqrt(jnp.mean(wide * wide, axis=-1, keepdims=True) + 1e-06)
        normed_ref[part, :] = (wide * inv * gain_ref[...]).astype(jnp.bfloat16)

    both = jnp.zeros((rows, 2 * mine), jnp.float32)
    for n in range(PIECES):
        part = slice(n * depth, (n + 1) * depth)
        copies[pieces + 2 * n].wait()
        copies[pieces + 2 * n + 1].wait()
        both += jnp.dot(normed_ref[:, part], wkv_ref[part, :], preferred_element_type=jnp.float32)
    k, v = both[:, :mine], both[:, mine:]
    upper = x % 2 == 1
    lane = lax.broadcasted_iota(jnp.int32, k.shape, 1)
    k_side = jnp.where(upper, pltpu.roll(k, HEAD_DIM, 1), k)
    v_side = jnp.where(upper, v, pltpu.roll(v, HEAD_DIM, 1))
    kv = jnp.where(lane < HEAD_DIM, k_side, v_side)
    turn_ref[...] = kv
    few = kv_ref.shape[0] // 2
    for odd in range(2):
        first = turn_ref[pl.ds(odd, few, stride=2), :]
        second = turn_ref[pl.ds(2 * few + odd, few, stride=2), :]
        part = slice(odd * few, (odd + 1) * few)
        kv_ref[part, :] = jnp.where(lax.axis_index("c") == 0, first, second).astype(jnp.bfloat16)

    q = jnp.zeros((rows, mine), jnp.float32)
    for n in range(PIECES):
        part = slice(n * depth, (n + 1) * depth)
        copies[pieces + 2 * PIECES + n].wait()
        q += jnp.dot(normed_ref[:, part], wq_ref[part, :], preferred_element_type=jnp.float32)
    q = q.astype(jnp.bfloat16) * jnp.bfloat16(HEAD_DIM**-0.5)
    for dest in range(q_ref.shape[0]):
        q_ref[dest] = q


def attend_kernel(bias_ref, q_ref, kv_ref, out_ref, qs, evens, odds, acc, carry):
    cores, places, half = kv_ref.shape[:3]
    blocks, tok = q_ref.shape[0], q_ref.shape[1]
    mine = 2 * HEAD_DIM
    few, wide = half // 2, TILE // 2
    key_tiles = places * tok // TILE
    tokens = blocks * tok
    row_tiles = tokens // TILE
    lane = lax.broadcasted_iota(jnp.int32, (tok, mine), 1)
    for b in range(blocks):
        q = q_ref[b].astype(jnp.float32)
        qs[b * tok : (b + 1) * tok, :] = jnp.where(lane < HEAD_DIM, q, 0.0).astype(jnp.bfloat16)
        turned = jnp.where(lane < HEAD_DIM, pltpu.roll(q, HEAD_DIM, 1), 0.0)
        qs[tokens + b * tok : tokens + (b + 1) * tok, :] = turned.astype(jnp.bfloat16)
    own = lax.axis_index("y")
    span = len(NEAR)
    for row in range(span):
        for turn in range(span):
            source = lax.rem(span * own + NEAR[row][turn] + places, places)
            place = row * span + lax.rem(own + turn, span)
            for core in range(cores):
                at = pl.multiple_of(place * (tok // 2) + core * few, 16)
                evens[pl.ds(at, few), :] = kv_ref[core, source, :few, :]
                odds[pl.ds(at, few), :] = kv_ref[core, source, few:, :]
    acc[...] = jnp.zeros_like(acc)
    carry[...] = jnp.full(carry.shape, -HELD, jnp.float32)
    from_row = lax.broadcasted_iota(jnp.int32, (TILE, TILE), 0)
    to_col = lax.broadcasted_iota(jnp.int32, (TILE, TILE), 1)
    in_half = (from_row < wide) == (to_col < wide)
    later_pair = ((from_row > to_col) & in_half).astype(jnp.bfloat16)

    def order(lanes):
        return jnp.where(lanes < wide, 2 * lanes, 2 * (lanes - wide) + 1)

    later = (order(from_row) > order(to_col)).astype(jnp.bfloat16)
    rel = lax.axis_index("z") * row_tiles - own * key_tiles

    keep_row = lax.broadcasted_iota(jnp.int32, (mine, mine), 0)
    keys_only = (keep_row < HEAD_DIM).astype(jnp.bfloat16)

    def largest(rows):
        square = rows.astype(jnp.float32)
        square = (square * square).astype(jnp.bfloat16)
        return jnp.max(jnp.dot(square, keys_only, preferred_element_type=jnp.float32))

    key_norm = jnp.maximum(largest(evens[...]), largest(odds[...]))
    room = 20.0 - jnp.maximum(bias_ref[0], bias_ref[1])
    tame = (room > 0.0) & (largest(qs[...]) * key_norm * 1.03 <= room * room)

    def tile(k):
        at = pl.ds(pl.multiple_of(k * wide, wide), wide)
        kv = jnp.concatenate([evens[at, :], odds[at, :]], axis=0)
        raw = lax.dot_general(
            qs[...], kv, (((1,), (1,)), ((), ())), preferred_element_type=jnp.float32
        )
        return kv, jnp.concatenate([raw[:tokens] + bias_ref[0], raw[tokens:] + bias_ref[1]], axis=0)

    def step(k, masked):
        kv, z = tile(k)
        if masked:
            t = lax.broadcasted_iota(jnp.int32, (tokens, TILE), 0)
            s = order(lax.broadcasted_iota(jnp.int32, (tokens, TILE), 1)) + (k - rel) * TILE
            seen = jnp.concatenate([s < t, s < t], axis=0)
            z = jnp.where(seen, z, -1e30)
        soft = jnp.maximum(z, jnp.log(1.0 + jnp.exp(jnp.minimum(z, 80.0))))
        between = jnp.dot(soft.astype(jnp.bfloat16), later, preferred_element_type=jnp.float32)
        held = carry[...]
        weight = jnp.exp((z - soft) - between - jnp.concatenate([held, held], axis=1))
        acc[...] += jnp.dot(weight.astype(jnp.bfloat16), kv, preferred_element_type=jnp.float32)
        carry[...] = held + jnp.broadcast_to(between[:, :1] + soft[:, :1], held.shape)

    def tame_step(k):
        kv, z = tile(k)
        u = jnp.exp(z)
        u_even, u_odd = u[:, :wide], u[:, wide:]
        even = 1.0 + u_even
        pair = even * (1.0 + u_odd)
        soft = jnp.log(pair)
        short = soft.astype(jnp.bfloat16)
        both = jnp.dot(
            jnp.concatenate([short[:tokens], short[tokens:]], axis=1),
            later_pair,
            preferred_element_type=jnp.float32,
        )
        between = jnp.concatenate([both[:, :wide], both[:, wide:]], axis=0)
        held = carry[...]
        rest = jnp.exp(-(between + held)) / pair
        weight = jnp.concatenate(
            [(u_even * rest).astype(jnp.bfloat16), (u_odd * even * rest).astype(jnp.bfloat16)], axis=1
        )
        acc[...] += jnp.dot(weight, kv, preferred_element_type=jnp.float32)
        carry[...] = held + jnp.broadcast_to(between[:, :1] + soft[:, :1], held.shape)

    @pl.when((rel >= 0) & (rel < key_tiles))
    def _():
        @pl.loop(0, row_tiles)
        def _(n):
            step(rel + row_tiles - 1 - n, True)

    whole = jnp.clip(rel, 0, key_tiles)

    @pl.when(tame)
    def _():
        @pl.loop(0, whole // row_tiles)
        def _(n):
            for m in range(row_tiles):
                tame_step(whole - 1 - row_tiles * n - m)

    @pl.when(jnp.logical_not(tame))
    def _():
        @pl.loop(0, whole)
        def _(n):
            step(whole - 1 - n, False)

    mark_row = lax.broadcasted_iota(jnp.int32, (16, mine), 0)
    mark_lane = lax.broadcasted_iota(jnp.int32, (16, mine), 1)
    pick = (mark_row * HEAD_DIM == mark_lane) & (mark_row < 2)
    pick = pick.astype(jnp.bfloat16)
    for n in range(blocks):
        first = slice(n * tok, (n + 1) * tok)
        second = slice(tokens + n * tok, tokens + (n + 1) * tok)
        part = jnp.where(lane < HEAD_DIM, pltpu.roll(acc[first], HEAD_DIM, 1), acc[second]) * 2.0**-64
        decay = jnp.exp(-(jnp.where(lane < HEAD_DIM, carry[first], carry[second]) + HELD))
        out_ref[n, :tok, :] = part.astype(jnp.bfloat16)
        turned = lax.dot_general(
            pick, decay.astype(jnp.bfloat16), (((1,), (1,)), ((), ())), preferred_element_type=jnp.float32
        ).astype(jnp.bfloat16)
        out_ref[n, tok : tok + 16, :] = turned[:, :mine]
        out_ref[n, tok + 16 :, :] = jnp.zeros((16, mine), jnp.bfloat16)
        out_ref[n, tok + 16 :, : tok - mine] = turned[:, mine:]


def combine_kernel(part_ref, out_ref):
    tok, mine = out_ref.shape[1], out_ref.shape[2]
    row = lax.broadcasted_iota(jnp.int32, (16, mine), 0)
    lane = lax.broadcasted_iota(jnp.int32, (16, mine), 1)
    spread = (row == lane // HEAD_DIM).astype(jnp.bfloat16)

    def column(turned):
        return lax.dot_general(
            turned, spread, (((0,), (0,)), ((), ())), preferred_element_type=jnp.float32
        )

    total = part_ref[0, :tok].astype(jnp.float32)
    for n in range(1, part_ref.shape[0]):
        decay = jnp.concatenate(
            [
                column(part_ref[n, tok : tok + 16, :]),
                column(part_ref[n, tok + 16 :, :])[: tok - mine],
            ],
            axis=0,
        )
        total = part_ref[n, :tok].astype(jnp.float32) + decay * total
    attended = total.astype(jnp.bfloat16)
    for dest in range(out_ref.shape[0]):
        out_ref[dest] = attended


def project_out_kernel(heads_ref, own_ref, other_ref, out_ref, joined):
    c = lax.axis_index("c")
    xs, mine = own_ref.shape[0], own_ref.shape[1]
    for side, core in enumerate((c, 1 - c)):
        for x in range(xs):
            col = (side * xs + x) * mine
            joined[:, col : col + mine] = heads_ref[2 * x + core]
    half = xs * mine
    block = 512
    for n in range(out_ref.shape[1] // block):
        cols = slice(n * block, (n + 1) * block)
        total = jnp.dot(
            joined[:, :half], own_ref[:, :, cols].reshape(half, block), preferred_element_type=jnp.float32
        )
        total += jnp.dot(
            joined[:, half:], other_ref[:, :, cols].reshape(half, block), preferred_element_type=jnp.float32
        )
        out_ref[:, cols] = total.astype(jnp.bfloat16)


def local(hidden, norm_gain, query_weight, key_weight, value_weight, head_bias, output_weight):
    rows, width = hidden.shape
    zs, ys, xs = lax.axis_size("z"), lax.axis_size("y"), lax.axis_size("x")
    cores = lax.axis_size("c")
    tps = xs * cores
    mine = 2 * HEAD_DIM
    vmem = pl.BlockSpec(memory_space=VMEM)
    smem = pl.BlockSpec(memory_space=SMEM)
    anywhere = pl.BlockSpec(memory_space=pl.ANY)

    queries, kv = pl.pallas_call(
        project_kernel,
        in_specs=[anywhere, vmem, anywhere, anywhere, anywhere],
        out_specs=[vmem, vmem],
        out_shape=[
            jax.ShapeDtypeStruct((ys, rows, mine), jnp.bfloat16),
            jax.ShapeDtypeStruct((rows // cores, mine), jnp.bfloat16),
        ],
        scratch_shapes=[
            VMEM((rows, width), jnp.bfloat16),
            VMEM((width, mine), jnp.bfloat16),
            VMEM((width, 2 * mine), jnp.bfloat16),
            VMEM((rows, width), jnp.bfloat16),
            VMEM((rows, mine), jnp.float32),
            pltpu.SemaphoreType.DMA((rows // ROWS_AT_ONCE + 3 * PIECES,)),
        ],
        compiler_params=pltpu.CompilerParams(vmem_limit_bytes=LIMIT),
        cost_estimate=pl.CostEstimate(
            flops=2 * rows * width * 3 * mine,
            bytes_accessed=2 * width * (rows + 3 * mine),
            transcendentals=0,
        ),
        name="project",
    )(hidden, norm_gain[None, :], query_weight, key_weight, value_weight)

    pairs = []
    for z in range(zs):
        for y in range(ys):
            super_row, row = divmod(z, ys)
            near = (ys * super_row + NEAR[row][(y - super_row) % ys]) % zs
            pairs.append((z * ys + y, near * ys + super_row))
    moved = lax.ppermute(kv, ("z", "y"), pairs)
    row_q = lax.all_to_all(queries, "y", 0, 0, tiled=True)
    fan = jnp.broadcast_to(output_weight[None], (xs, *output_weight.shape))
    row_q, moved, fan = lax.optimization_barrier((row_q, moved, fan))
    own_rows = lax.all_to_all(fan, "x", 0, 0, tiled=True)
    quarter_half = lax.all_gather(moved, "z", axis=0)
    quarter = lax.all_gather(quarter_half, "c", axis=0)
    quarter, own_rows = lax.optimization_barrier((quarter, own_rows))
    other_rows = lax.ppermute(own_rows, "c", [(0, 1), (1, 0)])

    tokens = ys * rows
    part = pl.pallas_call(
        attend_kernel,
        in_specs=[smem, vmem, vmem],
        out_specs=vmem,
        out_shape=jax.ShapeDtypeStruct((ys, rows + 32, mine), jnp.bfloat16),
        scratch_shapes=[
            VMEM((2 * tokens, mine), jnp.bfloat16),
            VMEM((zs * rows // 2, mine), jnp.bfloat16),
            VMEM((zs * rows // 2, mine), jnp.bfloat16),
            VMEM((2 * tokens, mine), jnp.float32),
            VMEM((2 * tokens, mine), jnp.float32),
        ],
        compiler_params=pltpu.CompilerParams(vmem_limit_bytes=24 * 1024 * 1024),
        cost_estimate=pl.CostEstimate(flops=10**10, bytes_accessed=2 * 10**6, transcendentals=0),
        name="attend",
    )(head_bias, row_q, quarter)

    parts = lax.all_to_all(part, "y", 0, 0, tiled=True)
    attended = pl.pallas_call(
        combine_kernel,
        in_specs=[vmem],
        out_specs=vmem,
        out_shape=jax.ShapeDtypeStruct((tps, rows, mine), jnp.bfloat16),
        compiler_params=pltpu.CompilerParams(vmem_limit_bytes=16 * 1024 * 1024),
        name="combine",
    )(parts)
    every_head = lax.all_to_all(attended, ("x", "c"), 0, 0, tiled=True)
    cols = output_weight.shape[1]
    return pl.pallas_call(
        project_out_kernel,
        in_specs=[vmem, vmem, vmem],
        out_specs=vmem,
        out_shape=jax.ShapeDtypeStruct((rows, cols), jnp.bfloat16),
        scratch_shapes=[VMEM((rows, tps * mine), jnp.bfloat16)],
        compiler_params=pltpu.CompilerParams(vmem_limit_bytes=20 * 1024 * 1024),
        cost_estimate=pl.CostEstimate(
            flops=2 * rows * tps * mine * cols, bytes_accessed=2 * tps * mine * cols, transcendentals=0
        ),
        name="project_out",
    )(every_head, own_rows, other_rows)


def solution(mesh):
    torus = Mesh(mesh.devices.reshape(16, 4, 4, 2), ("z", "y", "x", "c"))
    sp, tp = ("z", "y"), ("x", "c")
    in_specs = (P(sp, None), P(), P(None, tp), P(), P(), P(tp), P(tp, None))
    return jax.shard_map(
        local, mesh=torus, in_specs=in_specs, out_specs=P(sp, None), check_vma=False
    )
```

```python
import math

import jax
import jax.numpy as jnp
from jax import lax
from jax.experimental import pallas as pl
from jax.experimental.pallas import tpu as pltpu
from jax.sharding import Mesh
from jax.sharding import PartitionSpec as P


HEAD_DIM = 64
TILE = 256
AT_ONCE = 6
VMEM = pltpu.VMEM
SMEM = pltpu.SMEM
HELD = 64 * math.log(2.0)


ROWS_AT_ONCE = 32
NEAR = ((-6, -5, -3, -4), (-2, -1, 1, 0), (5, 4, 2, 3), (9, 8, 6, 7))


def project_kernel(
    hidden_hbm,
    gain_hbm,
    wq_hbm,
    wk_hbm,
    wv_hbm,
    q_ref,
    kv_ref,
    hidden_ref,
    gain_ref,
    wq_ref,
    wkv_ref,
    normed_ref,
    turn_ref,
    sems,
):
    rows, _ = hidden_ref.shape
    mine = 2 * HEAD_DIM
    x = lax.axis_index("x")
    cols = pl.ds(pl.multiple_of((x // 2) * mine, mine), mine)
    pairs = (
        (gain_hbm, gain_ref),
        (hidden_hbm, hidden_ref),
        (wk_hbm.at[:, cols], wkv_ref.at[:, :mine]),
        (wv_hbm.at[:, cols], wkv_ref.at[:, mine:]),
        (wq_hbm, wq_ref),
    )
    copies = [pltpu.make_async_copy(src, dst, sems.at[n]) for n, (src, dst) in enumerate(pairs)]
    for copy in copies:
        copy.start()
    copies[0].wait()
    copies[1].wait()
    for n in range(rows // ROWS_AT_ONCE):
        part = slice(n * ROWS_AT_ONCE, (n + 1) * ROWS_AT_ONCE)
        wide = hidden_ref[part, :].astype(jnp.float32)
        inv = lax.rsqrt(jnp.mean(wide * wide, axis=-1, keepdims=True) + 1e-06)
        normed_ref[part, :] = (wide * inv * gain_ref[...]).astype(jnp.bfloat16)

    copies[2].wait()
    copies[3].wait()
    both = jnp.dot(normed_ref[...], wkv_ref[...], preferred_element_type=jnp.float32)
    k, v = both[:, :mine], both[:, mine:]
    upper = x % 2 == 1
    lane = lax.broadcasted_iota(jnp.int32, k.shape, 1)
    k_side = jnp.where(upper, pltpu.roll(k, HEAD_DIM, 1), k)
    v_side = jnp.where(upper, v, pltpu.roll(v, HEAD_DIM, 1))
    kv = jnp.where(lane < HEAD_DIM, k_side, v_side)
    turn_ref[...] = kv
    few = kv_ref.shape[0] // 2
    for odd in range(2):
        first = turn_ref[pl.ds(odd, few, stride=2), :]
        second = turn_ref[pl.ds(2 * few + odd, few, stride=2), :]
        part = slice(odd * few, (odd + 1) * few)
        kv_ref[part, :] = jnp.where(lax.axis_index("c") == 0, first, second).astype(jnp.bfloat16)

    copies[4].wait()
    q = jnp.dot(normed_ref[...], wq_ref[...], preferred_element_type=jnp.float32)
    q = q.astype(jnp.bfloat16) * jnp.bfloat16(HEAD_DIM**-0.5)
    for dest in range(q_ref.shape[0]):
        q_ref[dest] = q


def attend_kernel(bias_ref, q_ref, kv_ref, out_ref, qs, evens, odds, acc, carry):
    cores, places, half = kv_ref.shape[:3]
    blocks, tok = q_ref.shape[0], q_ref.shape[1]
    mine = 2 * HEAD_DIM
    few, wide = half // 2, TILE // 2
    key_tiles = places * tok // TILE
    tokens = blocks * tok
    row_tiles = tokens // TILE
    lane = lax.broadcasted_iota(jnp.int32, (tok, mine), 1)
    for b in range(blocks):
        q = q_ref[b].astype(jnp.float32)
        qs[b * tok : (b + 1) * tok, :] = jnp.where(lane < HEAD_DIM, q, 0.0).astype(jnp.bfloat16)
        turned = jnp.where(lane < HEAD_DIM, pltpu.roll(q, HEAD_DIM, 1), 0.0)
        qs[tokens + b * tok : tokens + (b + 1) * tok, :] = turned.astype(jnp.bfloat16)
    own = lax.axis_index("y")
    span = len(NEAR)
    for row in range(span):
        for turn in range(span):
            source = lax.rem(span * own + NEAR[row][turn] + places, places)
            place = row * span + lax.rem(own + turn, span)
            for core in range(cores):
                at = pl.multiple_of(place * (tok // 2) + core * few, 16)
                evens[pl.ds(at, few), :] = kv_ref[core, source, :few, :]
                odds[pl.ds(at, few), :] = kv_ref[core, source, few:, :]
    acc[...] = jnp.zeros_like(acc)
    carry[...] = jnp.full(carry.shape, -HELD, jnp.float32)
    from_row = lax.broadcasted_iota(jnp.int32, (TILE, TILE), 0)
    to_col = lax.broadcasted_iota(jnp.int32, (TILE, TILE), 1)
    in_half = (from_row < wide) == (to_col < wide)
    later_pair = ((from_row > to_col) & in_half).astype(jnp.bfloat16)

    def order(lanes):
        return jnp.where(lanes < wide, 2 * lanes, 2 * (lanes - wide) + 1)

    later = (order(from_row) > order(to_col)).astype(jnp.bfloat16)
    rel = lax.axis_index("z") * row_tiles - own * key_tiles

    keep_row = lax.broadcasted_iota(jnp.int32, (mine, mine), 0)
    keys_only = (keep_row < HEAD_DIM).astype(jnp.bfloat16)

    def largest(rows):
        square = rows.astype(jnp.float32)
        square = (square * square).astype(jnp.bfloat16)
        return jnp.max(jnp.dot(square, keys_only, preferred_element_type=jnp.float32))

    key_norm = jnp.maximum(largest(evens[...]), largest(odds[...]))
    room = 20.0 - jnp.maximum(bias_ref[0], bias_ref[1])
    tame = (room > 0.0) & (largest(qs[...]) * key_norm * 1.03 <= room * room)

    def tile(k):
        at = pl.ds(pl.multiple_of(k * wide, wide), wide)
        kv = jnp.concatenate([evens[at, :], odds[at, :]], axis=0)
        raw = lax.dot_general(
            qs[...], kv, (((1,), (1,)), ((), ())), preferred_element_type=jnp.float32
        )
        return kv, jnp.concatenate([raw[:tokens] + bias_ref[0], raw[tokens:] + bias_ref[1]], axis=0)

    def step(k, masked):
        kv, z = tile(k)
        if masked:
            t = lax.broadcasted_iota(jnp.int32, (tokens, TILE), 0)
            s = order(lax.broadcasted_iota(jnp.int32, (tokens, TILE), 1)) + (k - rel) * TILE
            seen = jnp.concatenate([s < t, s < t], axis=0)
            z = jnp.where(seen, z, -1e30)
        soft = jnp.maximum(z, jnp.log(1.0 + jnp.exp(jnp.minimum(z, 80.0))))
        between = jnp.dot(soft.astype(jnp.bfloat16), later, preferred_element_type=jnp.float32)
        held = carry[...]
        weight = jnp.exp((z - soft) - between - jnp.concatenate([held, held], axis=1))
        acc[...] += jnp.dot(weight.astype(jnp.bfloat16), kv, preferred_element_type=jnp.float32)
        carry[...] = held + jnp.broadcast_to(between[:, :1] + soft[:, :1], held.shape)

    def tame_step(k):
        kv, z = tile(k)
        u = jnp.exp(z)
        u_even, u_odd = u[:, :wide], u[:, wide:]
        even = 1.0 + u_even
        pair = even * (1.0 + u_odd)
        soft = jnp.log(pair)
        short = soft.astype(jnp.bfloat16)
        both = jnp.dot(
            jnp.concatenate([short[:tokens], short[tokens:]], axis=1),
            later_pair,
            preferred_element_type=jnp.float32,
        )
        between = jnp.concatenate([both[:, :wide], both[:, wide:]], axis=0)
        held = carry[...]
        rest = jnp.exp(-(between + held)) / pair
        weight = jnp.concatenate(
            [(u_even * rest).astype(jnp.bfloat16), (u_odd * even * rest).astype(jnp.bfloat16)], axis=1
        )
        acc[...] += jnp.dot(weight, kv, preferred_element_type=jnp.float32)
        carry[...] = held + jnp.broadcast_to(between[:, :1] + soft[:, :1], held.shape)

    @pl.when((rel >= 0) & (rel < key_tiles))
    def _():
        @pl.loop(0, row_tiles)
        def _(n):
            step(rel + row_tiles - 1 - n, True)

    whole = jnp.clip(rel, 0, key_tiles)

    @pl.when(tame)
    def _():
        @pl.loop(0, whole // AT_ONCE)
        def _(n):
            for m in range(AT_ONCE):
                tame_step(whole - 1 - AT_ONCE * n - m)

        left = lax.rem(whole, AT_ONCE)

        @pl.loop(0, left)
        def _(n):
            tame_step(left - 1 - n)

    @pl.when(jnp.logical_not(tame))
    def _():
        @pl.loop(0, whole)
        def _(n):
            step(whole - 1 - n, False)

    mark_row = lax.broadcasted_iota(jnp.int32, (16, mine), 0)
    mark_lane = lax.broadcasted_iota(jnp.int32, (16, mine), 1)
    pick = (mark_row * HEAD_DIM == mark_lane) & (mark_row < 2)
    pick = pick.astype(jnp.bfloat16)
    for n in range(blocks):
        first = slice(n * tok, (n + 1) * tok)
        second = slice(tokens + n * tok, tokens + (n + 1) * tok)
        part = jnp.where(lane < HEAD_DIM, pltpu.roll(acc[first], HEAD_DIM, 1), acc[second]) * 2.0**-64
        decay = jnp.exp(-(jnp.where(lane < HEAD_DIM, carry[first], carry[second]) + HELD))
        out_ref[n, :tok, :] = part.astype(jnp.bfloat16)
        turned = lax.dot_general(
            pick, decay.astype(jnp.bfloat16), (((1,), (1,)), ((), ())), preferred_element_type=jnp.float32
        ).astype(jnp.bfloat16)
        out_ref[n, tok : tok + 16, :] = turned[:, :mine]
        out_ref[n, tok + 16 :, :] = jnp.zeros((16, mine), jnp.bfloat16)
        out_ref[n, tok + 16 :, : tok - mine] = turned[:, mine:]


def combine_kernel(part_ref, out_ref):
    tok, mine = out_ref.shape[1], out_ref.shape[2]
    row = lax.broadcasted_iota(jnp.int32, (16, mine), 0)
    lane = lax.broadcasted_iota(jnp.int32, (16, mine), 1)
    spread = (row == lane // HEAD_DIM).astype(jnp.bfloat16)

    def column(turned):
        return lax.dot_general(
            turned, spread, (((0,), (0,)), ((), ())), preferred_element_type=jnp.float32
        )

    total = part_ref[0, :tok].astype(jnp.float32)
    for n in range(1, part_ref.shape[0]):
        decay = jnp.concatenate(
            [
                column(part_ref[n, tok : tok + 16, :]),
                column(part_ref[n, tok + 16 :, :])[: tok - mine],
            ],
            axis=0,
        )
        total = part_ref[n, :tok].astype(jnp.float32) + decay * total
    attended = total.astype(jnp.bfloat16)
    for dest in range(out_ref.shape[0]):
        out_ref[dest] = attended


def project_out_kernel(heads_ref, own_ref, other_ref, out_ref, joined):
    c = lax.axis_index("c")
    xs, mine = own_ref.shape[0], own_ref.shape[1]
    for side, core in enumerate((c, 1 - c)):
        for x in range(xs):
            col = (side * xs + x) * mine
            joined[:, col : col + mine] = heads_ref[2 * x + core]
    half = xs * mine
    block = 512
    for n in range(out_ref.shape[1] // block):
        cols = slice(n * block, (n + 1) * block)
        total = jnp.dot(
            joined[:, :half], own_ref[:, :, cols].reshape(half, block), preferred_element_type=jnp.float32
        )
        total += jnp.dot(
            joined[:, half:], other_ref[:, :, cols].reshape(half, block), preferred_element_type=jnp.float32
        )
        out_ref[:, cols] = total.astype(jnp.bfloat16)


def local(hidden, norm_gain, query_weight, key_weight, value_weight, head_bias, output_weight):
    rows, width = hidden.shape
    zs, ys, xs = lax.axis_size("z"), lax.axis_size("y"), lax.axis_size("x")
    cores = lax.axis_size("c")
    tps = xs * cores
    mine = 2 * HEAD_DIM
    vmem = pl.BlockSpec(memory_space=VMEM)
    smem = pl.BlockSpec(memory_space=SMEM)
    anywhere = pl.BlockSpec(memory_space=pl.ANY)

    queries, kv = pl.pallas_call(
        project_kernel,
        in_specs=[anywhere] * 5,
        out_specs=[vmem, vmem],
        out_shape=[
            jax.ShapeDtypeStruct((ys, rows, mine), jnp.bfloat16),
            jax.ShapeDtypeStruct((rows // cores, mine), jnp.bfloat16),
        ],
        scratch_shapes=[
            VMEM((rows, width), jnp.bfloat16),
            VMEM((1, width), jnp.float32),
            VMEM((width, mine), jnp.bfloat16),
            VMEM((width, 2 * mine), jnp.bfloat16),
            VMEM((rows, width), jnp.bfloat16),
            VMEM((rows, mine), jnp.float32),
            pltpu.SemaphoreType.DMA((5,)),
        ],
        compiler_params=pltpu.CompilerParams(vmem_limit_bytes=56 * 1024 * 1024),
        cost_estimate=pl.CostEstimate(
            flops=2 * rows * width * 3 * mine,
            bytes_accessed=2 * width * (rows + 3 * mine),
            transcendentals=0,
        ),
        name="project",
    )(hidden, norm_gain[None, :], query_weight, key_weight, value_weight)

    pairs = []
    for z in range(zs):
        for y in range(ys):
            super_row, row = divmod(z, ys)
            near = (ys * super_row + NEAR[row][(y - super_row) % ys]) % zs
            pairs.append((z * ys + y, near * ys + super_row))
    moved = lax.ppermute(kv, ("z", "y"), pairs)
    row_q = lax.all_to_all(queries, "y", 0, 0, tiled=True)
    fan = jnp.broadcast_to(output_weight[None], (xs, *output_weight.shape))
    row_q, moved, fan = lax.optimization_barrier((row_q, moved, fan))
    own_rows = lax.all_to_all(fan, "x", 0, 0, tiled=True)
    quarter_half = lax.all_gather(moved, "z", axis=0)
    quarter = lax.all_gather(quarter_half, "c", axis=0)
    quarter, own_rows = lax.optimization_barrier((quarter, own_rows))
    other_rows = lax.ppermute(own_rows, "c", [(0, 1), (1, 0)])

    tokens = ys * rows
    part = pl.pallas_call(
        attend_kernel,
        in_specs=[smem, vmem, vmem],
        out_specs=vmem,
        out_shape=jax.ShapeDtypeStruct((ys, rows + 32, mine), jnp.bfloat16),
        scratch_shapes=[
            VMEM((2 * tokens, mine), jnp.bfloat16),
            VMEM((zs * rows // 2, mine), jnp.bfloat16),
            VMEM((zs * rows // 2, mine), jnp.bfloat16),
            VMEM((2 * tokens, mine), jnp.float32),
            VMEM((2 * tokens, mine), jnp.float32),
        ],
        compiler_params=pltpu.CompilerParams(vmem_limit_bytes=24 * 1024 * 1024),
        cost_estimate=pl.CostEstimate(flops=10**10, bytes_accessed=2 * 10**6, transcendentals=0),
        name="attend",
    )(head_bias, row_q, quarter)

    parts = lax.all_to_all(part, "y", 0, 0, tiled=True)
    attended = pl.pallas_call(
        combine_kernel,
        in_specs=[vmem],
        out_specs=vmem,
        out_shape=jax.ShapeDtypeStruct((tps, rows, mine), jnp.bfloat16),
        compiler_params=pltpu.CompilerParams(vmem_limit_bytes=16 * 1024 * 1024),
        name="combine",
    )(parts)
    every_head = lax.all_to_all(attended, ("x", "c"), 0, 0, tiled=True)
    cols = output_weight.shape[1]
    return pl.pallas_call(
        project_out_kernel,
        in_specs=[vmem, vmem, vmem],
        out_specs=vmem,
        out_shape=jax.ShapeDtypeStruct((rows, cols), jnp.bfloat16),
        scratch_shapes=[VMEM((rows, tps * mine), jnp.bfloat16)],
        compiler_params=pltpu.CompilerParams(vmem_limit_bytes=20 * 1024 * 1024),
        cost_estimate=pl.CostEstimate(
            flops=2 * rows * tps * mine * cols, bytes_accessed=2 * tps * mine * cols, transcendentals=0
        ),
        name="project_out",
    )(every_head, own_rows, other_rows)


def solution(mesh):
    torus = Mesh(mesh.devices.reshape(16, 4, 4, 2), ("z", "y", "x", "c"))
    sp, tp = ("z", "y"), ("x", "c")
    in_specs = (P(sp, None), P(), P(None, tp), P(), P(), P(tp), P(tp, None))
    return jax.shard_map(
        local, mesh=torus, in_specs=in_specs, out_specs=P(sp, None), check_vma=False
    )
```

```python
import math

import jax
import jax.numpy as jnp
from jax import lax
from jax.experimental import pallas as pl
from jax.experimental.pallas import tpu as pltpu
from jax.sharding import Mesh
from jax.sharding import PartitionSpec as P


HEAD_DIM = 64
TILE = 256
AT_ONCE = 6
VMEM = pltpu.VMEM
SMEM = pltpu.SMEM
HELD = 64 * math.log(2.0)


ROWS_AT_ONCE = 32
NEAR = ((-6, -5, -3, -4), (-2, -1, 1, 0), (5, 4, 2, 3), (9, 8, 6, 7))


def project_kernel(
    hidden_hbm,
    gain_hbm,
    wq_hbm,
    wk_hbm,
    wv_hbm,
    q_ref,
    kv_ref,
    hidden_ref,
    gain_ref,
    wq_ref,
    wkv_ref,
    normed_ref,
    turn_ref,
    sems,
):
    rows, _ = hidden_ref.shape
    mine = 2 * HEAD_DIM
    x = lax.axis_index("x")
    cols = pl.ds(pl.multiple_of((x // 2) * mine, mine), mine)
    pairs = (
        (gain_hbm, gain_ref),
        (hidden_hbm, hidden_ref),
        (wk_hbm.at[:, cols], wkv_ref.at[:, :mine]),
        (wv_hbm.at[:, cols], wkv_ref.at[:, mine:]),
        (wq_hbm, wq_ref),
    )
    copies = [pltpu.make_async_copy(src, dst, sems.at[n]) for n, (src, dst) in enumerate(pairs)]
    for copy in copies:
        copy.start()
    copies[0].wait()
    copies[1].wait()
    for n in range(rows // ROWS_AT_ONCE):
        part = slice(n * ROWS_AT_ONCE, (n + 1) * ROWS_AT_ONCE)
        wide = hidden_ref[part, :].astype(jnp.float32)
        inv = lax.rsqrt(jnp.mean(wide * wide, axis=-1, keepdims=True) + 1e-06)
        normed_ref[part, :] = (wide * inv * gain_ref[...]).astype(jnp.bfloat16)

    copies[2].wait()
    copies[3].wait()
    both = jnp.dot(normed_ref[...], wkv_ref[...], preferred_element_type=jnp.float32)
    k, v = both[:, :mine], both[:, mine:]
    upper = x % 2 == 1
    lane = lax.broadcasted_iota(jnp.int32, k.shape, 1)
    k_side = jnp.where(upper, pltpu.roll(k, HEAD_DIM, 1), k)
    v_side = jnp.where(upper, v, pltpu.roll(v, HEAD_DIM, 1))
    kv = jnp.where(lane < HEAD_DIM, k_side, v_side)
    turn_ref[...] = kv
    few = kv_ref.shape[0] // 2
    for odd in range(2):
        first = turn_ref[pl.ds(odd, few, stride=2), :]
        second = turn_ref[pl.ds(2 * few + odd, few, stride=2), :]
        part = slice(odd * few, (odd + 1) * few)
        kv_ref[part, :] = jnp.where(lax.axis_index("c") == 0, first, second).astype(jnp.bfloat16)

    copies[4].wait()
    q = jnp.dot(normed_ref[...], wq_ref[...], preferred_element_type=jnp.float32)
    q = q.astype(jnp.bfloat16) * jnp.bfloat16(HEAD_DIM**-0.5)
    for dest in range(q_ref.shape[0]):
        q_ref[dest] = q


def attend_kernel(bias_ref, q_ref, kv_ref, out_ref, qs, evens, odds, acc, carry):
    cores, places, half = kv_ref.shape[:3]
    blocks, tok = q_ref.shape[0], q_ref.shape[1]
    mine = 2 * HEAD_DIM
    few, wide = half // 2, TILE // 2
    key_tiles = places * tok // TILE
    tokens = blocks * tok
    row_tiles = tokens // TILE
    lane = lax.broadcasted_iota(jnp.int32, (tok, mine), 1)
    for b in range(blocks):
        q = q_ref[b].astype(jnp.float32)
        qs[b * tok : (b + 1) * tok, :] = jnp.where(lane < HEAD_DIM, q, 0.0).astype(jnp.bfloat16)
        turned = jnp.where(lane < HEAD_DIM, pltpu.roll(q, HEAD_DIM, 1), 0.0)
        qs[tokens + b * tok : tokens + (b + 1) * tok, :] = turned.astype(jnp.bfloat16)
    own = lax.axis_index("y")
    span = len(NEAR)
    for row in range(span):
        for turn in range(span):
            source = lax.rem(span * own + NEAR[row][turn] + places, places)
            place = row * span + lax.rem(own + turn, span)
            for core in range(cores):
                at = pl.multiple_of(place * (tok // 2) + core * few, 16)
                evens[pl.ds(at, few), :] = kv_ref[core, source, :few, :]
                odds[pl.ds(at, few), :] = kv_ref[core, source, few:, :]
    acc[...] = jnp.zeros_like(acc)
    carry[...] = jnp.full(carry.shape, -HELD, jnp.float32)
    from_row = lax.broadcasted_iota(jnp.int32, (TILE, TILE), 0)
    to_col = lax.broadcasted_iota(jnp.int32, (TILE, TILE), 1)
    in_half = (from_row < wide) == (to_col < wide)
    later_pair = ((from_row > to_col) & in_half).astype(jnp.bfloat16)

    def order(lanes):
        return jnp.where(lanes < wide, 2 * lanes, 2 * (lanes - wide) + 1)

    later = (order(from_row) > order(to_col)).astype(jnp.bfloat16)
    rel = lax.axis_index("z") * row_tiles - own * key_tiles

    keep_row = lax.broadcasted_iota(jnp.int32, (mine, mine), 0)
    keys_only = (keep_row < HEAD_DIM).astype(jnp.bfloat16)

    def largest(rows):
        square = rows.astype(jnp.float32)
        square = (square * square).astype(jnp.bfloat16)
        return jnp.max(jnp.dot(square, keys_only, preferred_element_type=jnp.float32))

    key_norm = jnp.maximum(largest(evens[...]), largest(odds[...]))
    room = 20.0 - jnp.maximum(bias_ref[0], bias_ref[1])
    tame = (room > 0.0) & (largest(qs[...]) * key_norm * 1.03 <= room * room)

    def tile(k):
        at = pl.ds(pl.multiple_of(k * wide, wide), wide)
        kv = jnp.concatenate([evens[at, :], odds[at, :]], axis=0)
        raw = lax.dot_general(
            qs[...], kv, (((1,), (1,)), ((), ())), preferred_element_type=jnp.float32
        )
        return kv, jnp.concatenate([raw[:tokens] + bias_ref[0], raw[tokens:] + bias_ref[1]], axis=0)

    def shown(k, z):
        t = lax.broadcasted_iota(jnp.int32, (tokens, TILE), 0)
        s = order(lax.broadcasted_iota(jnp.int32, (tokens, TILE), 1))
        seen = s - t < (rel - k) * TILE
        return jnp.where(jnp.concatenate([seen, seen], axis=0), z, -1e30)

    def step(k, masked):
        kv, z = tile(k)
        if masked:
            z = shown(k, z)
        soft = jnp.maximum(z, jnp.log(1.0 + jnp.exp(jnp.minimum(z, 80.0))))
        between = jnp.dot(soft.astype(jnp.bfloat16), later, preferred_element_type=jnp.float32)
        held = carry[...]
        weight = jnp.exp((z - soft) - between - jnp.concatenate([held, held], axis=1))
        acc[...] += jnp.dot(weight.astype(jnp.bfloat16), kv, preferred_element_type=jnp.float32)
        carry[...] = held + jnp.broadcast_to(between[:, :1] + soft[:, :1], held.shape)

    def tame_step(k, masked):
        kv, z = tile(k)
        if masked:
            z = shown(k, z)
        u = jnp.exp(z)
        u_even, u_odd = u[:, :wide], u[:, wide:]
        even = 1.0 + u_even
        pair = even * (1.0 + u_odd)
        soft = jnp.log(pair)
        short = soft.astype(jnp.bfloat16)
        both = jnp.dot(
            jnp.concatenate([short[:tokens], short[tokens:]], axis=1),
            later_pair,
            preferred_element_type=jnp.float32,
        )
        between = jnp.concatenate([both[:, :wide], both[:, wide:]], axis=0)
        held = carry[...]
        rest = jnp.exp(-(between + held)) / pair
        weight = jnp.concatenate(
            [(u_even * rest).astype(jnp.bfloat16), (u_odd * even * rest).astype(jnp.bfloat16)], axis=1
        )
        acc[...] += jnp.dot(weight, kv, preferred_element_type=jnp.float32)
        carry[...] = held + jnp.broadcast_to(between[:, :1] + soft[:, :1], held.shape)

    crossed = (rel >= 0) & (rel < key_tiles)
    whole = jnp.clip(rel, 0, key_tiles)

    @pl.when(tame & crossed)
    def _():
        for m in range(row_tiles):
            tame_step(rel + row_tiles - 1 - m, True)

    @pl.when(tame)
    def _():
        @pl.loop(0, whole // AT_ONCE)
        def _(n):
            for m in range(AT_ONCE):
                tame_step(whole - 1 - AT_ONCE * n - m, False)

        @pl.when(lax.rem(whole, AT_ONCE) > 0)
        def _():
            for m in range(row_tiles):
                tame_step(row_tiles - 1 - m, False)

    @pl.when(jnp.logical_not(tame))
    def _():
        @pl.loop(0, jnp.where(crossed, row_tiles, 0))
        def _(n):
            step(rel + row_tiles - 1 - n, True)

        @pl.loop(0, whole)
        def _(n):
            step(whole - 1 - n, False)

    mark_row = lax.broadcasted_iota(jnp.int32, (16, mine), 0)
    mark_lane = lax.broadcasted_iota(jnp.int32, (16, mine), 1)
    pick = (mark_row * HEAD_DIM == mark_lane) & (mark_row < 2)
    pick = pick.astype(jnp.bfloat16)
    for n in range(blocks):
        first = slice(n * tok, (n + 1) * tok)
        second = slice(tokens + n * tok, tokens + (n + 1) * tok)
        part = jnp.where(lane < HEAD_DIM, pltpu.roll(acc[first], HEAD_DIM, 1), acc[second]) * 2.0**-64
        decay = jnp.exp(-(jnp.where(lane < HEAD_DIM, carry[first], carry[second]) + HELD))
        out_ref[n, :tok, :] = part.astype(jnp.bfloat16)
        turned = lax.dot_general(
            pick, decay.astype(jnp.bfloat16), (((1,), (1,)), ((), ())), preferred_element_type=jnp.float32
        ).astype(jnp.bfloat16)
        out_ref[n, tok : tok + 16, :] = turned[:, :mine]
        out_ref[n, tok + 16 :, :] = jnp.zeros((16, mine), jnp.bfloat16)
        out_ref[n, tok + 16 :, : tok - mine] = turned[:, mine:]


def combine_kernel(part_ref, out_ref):
    tok, mine = out_ref.shape[1], out_ref.shape[2]
    row = lax.broadcasted_iota(jnp.int32, (16, mine), 0)
    lane = lax.broadcasted_iota(jnp.int32, (16, mine), 1)
    spread = (row == lane // HEAD_DIM).astype(jnp.bfloat16)

    def column(turned):
        return lax.dot_general(
            turned, spread, (((0,), (0,)), ((), ())), preferred_element_type=jnp.float32
        )

    total = part_ref[0, :tok].astype(jnp.float32)
    for n in range(1, part_ref.shape[0]):
        decay = jnp.concatenate(
            [
                column(part_ref[n, tok : tok + 16, :]),
                column(part_ref[n, tok + 16 :, :])[: tok - mine],
            ],
            axis=0,
        )
        total = part_ref[n, :tok].astype(jnp.float32) + decay * total
    attended = total.astype(jnp.bfloat16)
    for dest in range(out_ref.shape[0]):
        out_ref[dest] = attended


def project_out_kernel(heads_ref, own_ref, other_ref, out_ref, joined):
    c = lax.axis_index("c")
    xs, mine = own_ref.shape[0], own_ref.shape[1]
    for side, core in enumerate((c, 1 - c)):
        for x in range(xs):
            col = (side * xs + x) * mine
            joined[:, col : col + mine] = heads_ref[2 * x + core]
    half = xs * mine
    block = 512
    for n in range(out_ref.shape[1] // block):
        cols = slice(n * block, (n + 1) * block)
        total = jnp.dot(
            joined[:, :half], own_ref[:, :, cols].reshape(half, block), preferred_element_type=jnp.float32
        )
        total += jnp.dot(
            joined[:, half:], other_ref[:, :, cols].reshape(half, block), preferred_element_type=jnp.float32
        )
        out_ref[:, cols] = total.astype(jnp.bfloat16)


def local(hidden, norm_gain, query_weight, key_weight, value_weight, head_bias, output_weight):
    rows, width = hidden.shape
    zs, ys, xs = lax.axis_size("z"), lax.axis_size("y"), lax.axis_size("x")
    cores = lax.axis_size("c")
    tps = xs * cores
    mine = 2 * HEAD_DIM
    vmem = pl.BlockSpec(memory_space=VMEM)
    smem = pl.BlockSpec(memory_space=SMEM)
    anywhere = pl.BlockSpec(memory_space=pl.ANY)

    queries, kv = pl.pallas_call(
        project_kernel,
        in_specs=[anywhere] * 5,
        out_specs=[vmem, vmem],
        out_shape=[
            jax.ShapeDtypeStruct((ys, rows, mine), jnp.bfloat16),
            jax.ShapeDtypeStruct((rows // cores, mine), jnp.bfloat16),
        ],
        scratch_shapes=[
            VMEM((rows, width), jnp.bfloat16),
            VMEM((1, width), jnp.float32),
            VMEM((width, mine), jnp.bfloat16),
            VMEM((width, 2 * mine), jnp.bfloat16),
            VMEM((rows, width), jnp.bfloat16),
            VMEM((rows, mine), jnp.float32),
            pltpu.SemaphoreType.DMA((5,)),
        ],
        compiler_params=pltpu.CompilerParams(vmem_limit_bytes=56 * 1024 * 1024),
        cost_estimate=pl.CostEstimate(
            flops=2 * rows * width * 3 * mine,
            bytes_accessed=2 * width * (rows + 3 * mine),
            transcendentals=0,
        ),
        name="project",
    )(hidden, norm_gain[None, :], query_weight, key_weight, value_weight)

    pairs = []
    for z in range(zs):
        for y in range(ys):
            super_row, row = divmod(z, ys)
            near = (ys * super_row + NEAR[row][(y - super_row) % ys]) % zs
            pairs.append((z * ys + y, near * ys + super_row))
    moved = lax.ppermute(kv, ("z", "y"), pairs)
    row_q = lax.all_to_all(queries, "y", 0, 0, tiled=True)
    fan = jnp.broadcast_to(output_weight[None], (xs, *output_weight.shape))
    row_q, moved, fan = lax.optimization_barrier((row_q, moved, fan))
    own_rows = lax.all_to_all(fan, "x", 0, 0, tiled=True)
    quarter_half = lax.all_gather(moved, "z", axis=0)
    quarter = lax.all_gather(quarter_half, "c", axis=0)
    quarter, own_rows = lax.optimization_barrier((quarter, own_rows))
    other_rows = lax.ppermute(own_rows, "c", [(0, 1), (1, 0)])

    tokens = ys * rows
    part = pl.pallas_call(
        attend_kernel,
        in_specs=[smem, vmem, vmem],
        out_specs=vmem,
        out_shape=jax.ShapeDtypeStruct((ys, rows + 32, mine), jnp.bfloat16),
        scratch_shapes=[
            VMEM((2 * tokens, mine), jnp.bfloat16),
            VMEM((zs * rows // 2, mine), jnp.bfloat16),
            VMEM((zs * rows // 2, mine), jnp.bfloat16),
            VMEM((2 * tokens, mine), jnp.float32),
            VMEM((2 * tokens, mine), jnp.float32),
        ],
        compiler_params=pltpu.CompilerParams(vmem_limit_bytes=24 * 1024 * 1024),
        cost_estimate=pl.CostEstimate(flops=10**10, bytes_accessed=2 * 10**6, transcendentals=0),
        name="attend",
    )(head_bias, row_q, quarter)

    parts = lax.all_to_all(part, "y", 0, 0, tiled=True)
    attended = pl.pallas_call(
        combine_kernel,
        in_specs=[vmem],
        out_specs=vmem,
        out_shape=jax.ShapeDtypeStruct((tps, rows, mine), jnp.bfloat16),
        compiler_params=pltpu.CompilerParams(vmem_limit_bytes=16 * 1024 * 1024),
        name="combine",
    )(parts)
    every_head = lax.all_to_all(attended, ("x", "c"), 0, 0, tiled=True)
    cols = output_weight.shape[1]
    return pl.pallas_call(
        project_out_kernel,
        in_specs=[vmem, vmem, vmem],
        out_specs=vmem,
        out_shape=jax.ShapeDtypeStruct((rows, cols), jnp.bfloat16),
        scratch_shapes=[VMEM((rows, tps * mine), jnp.bfloat16)],
        compiler_params=pltpu.CompilerParams(vmem_limit_bytes=20 * 1024 * 1024),
        cost_estimate=pl.CostEstimate(
            flops=2 * rows * tps * mine * cols, bytes_accessed=2 * tps * mine * cols, transcendentals=0
        ),
        name="project_out",
    )(every_head, own_rows, other_rows)


def solution(mesh):
    torus = Mesh(mesh.devices.reshape(16, 4, 4, 2), ("z", "y", "x", "c"))
    sp, tp = ("z", "y"), ("x", "c")
    in_specs = (P(sp, None), P(), P(None, tp), P(), P(), P(tp), P(tp, None))
    return jax.shard_map(
        local, mesh=torus, in_specs=in_specs, out_specs=P(sp, None), check_vma=False
    )
```

```python
import math

import jax
import jax.numpy as jnp
from jax import lax
from jax.experimental import pallas as pl
from jax.experimental.pallas import tpu as pltpu
from jax.sharding import Mesh
from jax.sharding import PartitionSpec as P


HEAD_DIM = 64
TILE = 256
AT_ONCE = 6
VMEM = pltpu.VMEM
SMEM = pltpu.SMEM
HELD = 64 * math.log(2.0)


ROWS_AT_ONCE = 32
NEAR = ((-6, -5, -3, -4), (-2, -1, 1, 0), (5, 4, 2, 3), (9, 8, 6, 7))


def project_kernel(
    hidden_hbm,
    gain_hbm,
    wq_hbm,
    wk_hbm,
    wv_hbm,
    q_ref,
    kv_ref,
    hidden_ref,
    gain_ref,
    wq_ref,
    wkv_ref,
    normed_ref,
    turn_ref,
    sems,
):
    rows, _ = hidden_ref.shape
    mine = 2 * HEAD_DIM
    x = lax.axis_index("x")
    cols = pl.ds(pl.multiple_of((x // 2) * mine, mine), mine)
    pairs = (
        (gain_hbm, gain_ref),
        (hidden_hbm, hidden_ref),
        (wk_hbm.at[:, cols], wkv_ref.at[:, :mine]),
        (wv_hbm.at[:, cols], wkv_ref.at[:, mine:]),
        (wq_hbm, wq_ref),
    )
    copies = [pltpu.make_async_copy(src, dst, sems.at[n]) for n, (src, dst) in enumerate(pairs)]
    for copy in copies:
        copy.start()
    copies[0].wait()
    copies[1].wait()
    for n in range(rows // ROWS_AT_ONCE):
        part = slice(n * ROWS_AT_ONCE, (n + 1) * ROWS_AT_ONCE)
        wide = hidden_ref[part, :].astype(jnp.float32)
        inv = lax.rsqrt(jnp.mean(wide * wide, axis=-1, keepdims=True) + 1e-06)
        normed_ref[part, :] = (wide * inv * gain_ref[...]).astype(jnp.bfloat16)

    copies[2].wait()
    copies[3].wait()
    both = jnp.dot(normed_ref[...], wkv_ref[...], preferred_element_type=jnp.float32)
    k, v = both[:, :mine], both[:, mine:]
    upper = x % 2 == 1
    lane = lax.broadcasted_iota(jnp.int32, k.shape, 1)
    k_side = jnp.where(upper, pltpu.roll(k, HEAD_DIM, 1), k)
    v_side = jnp.where(upper, v, pltpu.roll(v, HEAD_DIM, 1))
    kv = jnp.where(lane < HEAD_DIM, k_side, v_side)
    turn_ref[...] = kv
    few = kv_ref.shape[0] // 2
    for odd in range(2):
        first = turn_ref[pl.ds(odd, few, stride=2), :]
        second = turn_ref[pl.ds(2 * few + odd, few, stride=2), :]
        part = slice(odd * few, (odd + 1) * few)
        kv_ref[part, :] = jnp.where(lax.axis_index("c") == 0, first, second).astype(jnp.bfloat16)

    copies[4].wait()
    q = jnp.dot(normed_ref[...], wq_ref[...], preferred_element_type=jnp.float32)
    q = q.astype(jnp.bfloat16) * jnp.bfloat16(HEAD_DIM**-0.5)
    for dest in range(q_ref.shape[0]):
        q_ref[dest] = q


def attend_kernel(bias_ref, q_ref, kv_ref, out_ref, qs, evens, odds, acc, carry):
    cores, places, half = kv_ref.shape[:3]
    blocks, tok = q_ref.shape[0], q_ref.shape[1]
    mine = 2 * HEAD_DIM
    few, wide = half // 2, TILE // 2
    key_tiles = places * tok // TILE
    tokens = blocks * tok
    row_tiles = tokens // TILE
    lane = lax.broadcasted_iota(jnp.int32, (tok, mine), 1)
    for b in range(blocks):
        q = q_ref[b].astype(jnp.float32)
        qs[b * tok : (b + 1) * tok, :] = jnp.where(lane < HEAD_DIM, q, 0.0).astype(jnp.bfloat16)
        turned = jnp.where(lane < HEAD_DIM, pltpu.roll(q, HEAD_DIM, 1), 0.0)
        qs[tokens + b * tok : tokens + (b + 1) * tok, :] = turned.astype(jnp.bfloat16)
    own = lax.axis_index("y")
    span = len(NEAR)
    for row in range(span):
        for turn in range(span):
            source = lax.rem(span * own + NEAR[row][turn] + places, places)
            place = row * span + lax.rem(own + turn, span)
            for core in range(cores):
                at = pl.multiple_of(place * (tok // 2) + core * few, 16)
                evens[pl.ds(at, few), :] = kv_ref[core, source, :few, :]
                odds[pl.ds(at, few), :] = kv_ref[core, source, few:, :]
    acc[...] = jnp.zeros_like(acc)
    carry[...] = jnp.full(carry.shape, -HELD, jnp.float32)
    from_row = lax.broadcasted_iota(jnp.int32, (TILE, TILE), 0)
    to_col = lax.broadcasted_iota(jnp.int32, (TILE, TILE), 1)
    in_half = (from_row < wide) == (to_col < wide)
    later_pair = ((from_row > to_col) & in_half).astype(jnp.bfloat16)

    def order(lanes):
        return jnp.where(lanes < wide, 2 * lanes, 2 * (lanes - wide) + 1)

    later = (order(from_row) > order(to_col)).astype(jnp.bfloat16)
    rel = lax.axis_index("z") * row_tiles - own * key_tiles

    side = lax.broadcasted_iota(jnp.int32, (2 * mine, mine), 1) // HEAD_DIM
    place = lax.broadcasted_iota(jnp.int32, (2 * mine, mine), 0) // HEAD_DIM
    by_head = (place == side)[:mine].astype(jnp.bfloat16)
    by_key = (place == 2 * side).astype(jnp.bfloat16)

    def largest(rows, groups):
        return jnp.max(jnp.dot(rows * rows, groups, preferred_element_type=jnp.float32))

    key_norm = largest(jnp.concatenate([evens[...], odds[...]], axis=1), by_key)
    query_norm = largest(q_ref[...].reshape(tokens, mine), by_head)
    room = 20.0 - jnp.maximum(bias_ref[0], bias_ref[1])
    tame = (room > 0.0) & (query_norm * key_norm * 1.03 <= room * room)

    def tile(k):
        at = pl.ds(pl.multiple_of(k * wide, wide), wide)
        kv = jnp.concatenate([evens[at, :], odds[at, :]], axis=0)
        raw = lax.dot_general(
            qs[...], kv, (((1,), (1,)), ((), ())), preferred_element_type=jnp.float32
        )
        return kv, jnp.concatenate([raw[:tokens] + bias_ref[0], raw[tokens:] + bias_ref[1]], axis=0)

    def shown(k, z):
        t = lax.broadcasted_iota(jnp.int32, (tokens, TILE), 0)
        s = order(lax.broadcasted_iota(jnp.int32, (tokens, TILE), 1))
        seen = s - t < (rel - k) * TILE
        return jnp.where(jnp.concatenate([seen, seen], axis=0), z, -1e30)

    def step(k, masked):
        kv, z = tile(k)
        if masked:
            z = shown(k, z)
        soft = jnp.maximum(z, jnp.log(1.0 + jnp.exp(jnp.minimum(z, 80.0))))
        between = jnp.dot(soft.astype(jnp.bfloat16), later, preferred_element_type=jnp.float32)
        held = carry[...]
        weight = jnp.exp((z - soft) - between - jnp.concatenate([held, held], axis=1))
        acc[...] += jnp.dot(weight.astype(jnp.bfloat16), kv, preferred_element_type=jnp.float32)
        carry[...] = held + jnp.broadcast_to(between[:, :1] + soft[:, :1], held.shape)

    def tame_step(k, masked):
        kv, z = tile(k)
        if masked:
            z = shown(k, z)
        u = jnp.exp(z)
        u_even, u_odd = u[:, :wide], u[:, wide:]
        even = 1.0 + u_even
        pair = even * (1.0 + u_odd)
        soft = jnp.log(pair)
        short = soft.astype(jnp.bfloat16)
        both = jnp.dot(
            jnp.concatenate([short[:tokens], short[tokens:]], axis=1),
            later_pair,
            preferred_element_type=jnp.float32,
        )
        between = jnp.concatenate([both[:, :wide], both[:, wide:]], axis=0)
        held = carry[...]
        rest = jnp.exp(-(between + held)) / pair
        weight = jnp.concatenate(
            [(u_even * rest).astype(jnp.bfloat16), (u_odd * even * rest).astype(jnp.bfloat16)], axis=1
        )
        acc[...] += jnp.dot(weight, kv, preferred_element_type=jnp.float32)
        carry[...] = held + jnp.broadcast_to(between[:, :1] + soft[:, :1], held.shape)

    crossed = (rel >= 0) & (rel < key_tiles)
    whole = jnp.clip(rel, 0, key_tiles)

    @pl.when(tame & crossed)
    def _():
        for m in range(row_tiles):
            tame_step(rel + row_tiles - 1 - m, True)

    @pl.when(tame)
    def _():
        @pl.loop(0, whole // AT_ONCE)
        def _(n):
            for m in range(AT_ONCE):
                tame_step(whole - 1 - AT_ONCE * n - m, False)

        @pl.when(lax.rem(whole, AT_ONCE) > 0)
        def _():
            for m in range(row_tiles):
                tame_step(row_tiles - 1 - m, False)

    @pl.when(jnp.logical_not(tame))
    def _():
        @pl.loop(0, jnp.where(crossed, row_tiles, 0))
        def _(n):
            step(rel + row_tiles - 1 - n, True)

        @pl.loop(0, whole)
        def _(n):
            step(whole - 1 - n, False)

    mark_row = lax.broadcasted_iota(jnp.int32, (16, mine), 0)
    mark_lane = lax.broadcasted_iota(jnp.int32, (16, mine), 1)
    pick = (mark_row * HEAD_DIM == mark_lane) & (mark_row < 2)
    pick = pick.astype(jnp.bfloat16)
    for n in range(blocks):
        first = slice(n * tok, (n + 1) * tok)
        second = slice(tokens + n * tok, tokens + (n + 1) * tok)
        part = jnp.where(lane < HEAD_DIM, pltpu.roll(acc[first], HEAD_DIM, 1), acc[second]) * 2.0**-64
        decay = jnp.exp(-(jnp.where(lane < HEAD_DIM, carry[first], carry[second]) + HELD))
        out_ref[n, :tok, :] = part.astype(jnp.bfloat16)
        turned = lax.dot_general(
            pick, decay.astype(jnp.bfloat16), (((1,), (1,)), ((), ())), preferred_element_type=jnp.float32
        ).astype(jnp.bfloat16)
        out_ref[n, tok : tok + 16, :] = turned[:, :mine]
        out_ref[n, tok + 16 :, :] = jnp.zeros((16, mine), jnp.bfloat16)
        out_ref[n, tok + 16 :, : tok - mine] = turned[:, mine:]


def combine_kernel(part_ref, out_ref):
    tok, mine = out_ref.shape[1], out_ref.shape[2]
    row = lax.broadcasted_iota(jnp.int32, (16, mine), 0)
    lane = lax.broadcasted_iota(jnp.int32, (16, mine), 1)
    spread = (row == lane // HEAD_DIM).astype(jnp.bfloat16)

    def column(turned):
        return lax.dot_general(
            turned, spread, (((0,), (0,)), ((), ())), preferred_element_type=jnp.float32
        )

    total = part_ref[0, :tok].astype(jnp.float32)
    for n in range(1, part_ref.shape[0]):
        decay = jnp.concatenate(
            [
                column(part_ref[n, tok : tok + 16, :]),
                column(part_ref[n, tok + 16 :, :])[: tok - mine],
            ],
            axis=0,
        )
        total = part_ref[n, :tok].astype(jnp.float32) + decay * total
    attended = total.astype(jnp.bfloat16)
    for dest in range(out_ref.shape[0]):
        out_ref[dest] = attended


def project_out_kernel(heads_ref, own_ref, other_ref, out_ref, joined):
    c = lax.axis_index("c")
    xs, mine = own_ref.shape[0], own_ref.shape[1]
    for side, core in enumerate((c, 1 - c)):
        for x in range(xs):
            col = (side * xs + x) * mine
            joined[:, col : col + mine] = heads_ref[2 * x + core]
    half = xs * mine
    block = 512
    for n in range(out_ref.shape[1] // block):
        cols = slice(n * block, (n + 1) * block)
        total = jnp.dot(
            joined[:, :half], own_ref[:, :, cols].reshape(half, block), preferred_element_type=jnp.float32
        )
        total += jnp.dot(
            joined[:, half:], other_ref[:, :, cols].reshape(half, block), preferred_element_type=jnp.float32
        )
        out_ref[:, cols] = total.astype(jnp.bfloat16)


def local(hidden, norm_gain, query_weight, key_weight, value_weight, head_bias, output_weight):
    rows, width = hidden.shape
    zs, ys, xs = lax.axis_size("z"), lax.axis_size("y"), lax.axis_size("x")
    cores = lax.axis_size("c")
    tps = xs * cores
    mine = 2 * HEAD_DIM
    vmem = pl.BlockSpec(memory_space=VMEM)
    smem = pl.BlockSpec(memory_space=SMEM)
    anywhere = pl.BlockSpec(memory_space=pl.ANY)

    queries, kv = pl.pallas_call(
        project_kernel,
        in_specs=[anywhere] * 5,
        out_specs=[vmem, vmem],
        out_shape=[
            jax.ShapeDtypeStruct((ys, rows, mine), jnp.bfloat16),
            jax.ShapeDtypeStruct((rows // cores, mine), jnp.bfloat16),
        ],
        scratch_shapes=[
            VMEM((rows, width), jnp.bfloat16),
            VMEM((1, width), jnp.float32),
            VMEM((width, mine), jnp.bfloat16),
            VMEM((width, 2 * mine), jnp.bfloat16),
            VMEM((rows, width), jnp.bfloat16),
            VMEM((rows, mine), jnp.float32),
            pltpu.SemaphoreType.DMA((5,)),
        ],
        compiler_params=pltpu.CompilerParams(vmem_limit_bytes=56 * 1024 * 1024),
        cost_estimate=pl.CostEstimate(
            flops=2 * rows * width * 3 * mine,
            bytes_accessed=2 * width * (rows + 3 * mine),
            transcendentals=0,
        ),
        name="project",
    )(hidden, norm_gain[None, :], query_weight, key_weight, value_weight)

    pairs = []
    for z in range(zs):
        for y in range(ys):
            super_row, row = divmod(z, ys)
            near = (ys * super_row + NEAR[row][(y - super_row) % ys]) % zs
            pairs.append((z * ys + y, near * ys + super_row))
    moved = lax.ppermute(kv, ("z", "y"), pairs)
    row_q = lax.all_to_all(queries, "y", 0, 0, tiled=True)
    fan = jnp.broadcast_to(output_weight[None], (xs, *output_weight.shape))
    row_q, moved, fan = lax.optimization_barrier((row_q, moved, fan))
    own_rows = lax.all_to_all(fan, "x", 0, 0, tiled=True)
    quarter_half = lax.all_gather(moved, "z", axis=0)
    quarter = lax.all_gather(quarter_half, "c", axis=0)
    quarter, own_rows = lax.optimization_barrier((quarter, own_rows))
    other_rows = lax.ppermute(own_rows, "c", [(0, 1), (1, 0)])

    tokens = ys * rows
    part = pl.pallas_call(
        attend_kernel,
        in_specs=[smem, vmem, vmem],
        out_specs=vmem,
        out_shape=jax.ShapeDtypeStruct((ys, rows + 32, mine), jnp.bfloat16),
        scratch_shapes=[
            VMEM((2 * tokens, mine), jnp.bfloat16),
            VMEM((zs * rows // 2, mine), jnp.bfloat16),
            VMEM((zs * rows // 2, mine), jnp.bfloat16),
            VMEM((2 * tokens, mine), jnp.float32),
            VMEM((2 * tokens, mine), jnp.float32),
        ],
        compiler_params=pltpu.CompilerParams(vmem_limit_bytes=24 * 1024 * 1024),
        cost_estimate=pl.CostEstimate(flops=10**10, bytes_accessed=2 * 10**6, transcendentals=0),
        name="attend",
    )(head_bias, row_q, quarter)

    parts = lax.all_to_all(part, "y", 0, 0, tiled=True)
    attended = pl.pallas_call(
        combine_kernel,
        in_specs=[vmem],
        out_specs=vmem,
        out_shape=jax.ShapeDtypeStruct((tps, rows, mine), jnp.bfloat16),
        compiler_params=pltpu.CompilerParams(vmem_limit_bytes=16 * 1024 * 1024),
        name="combine",
    )(parts)
    every_head = lax.all_to_all(attended, ("x", "c"), 0, 0, tiled=True)
    cols = output_weight.shape[1]
    return pl.pallas_call(
        project_out_kernel,
        in_specs=[vmem, vmem, vmem],
        out_specs=vmem,
        out_shape=jax.ShapeDtypeStruct((rows, cols), jnp.bfloat16),
        scratch_shapes=[VMEM((rows, tps * mine), jnp.bfloat16)],
        compiler_params=pltpu.CompilerParams(vmem_limit_bytes=20 * 1024 * 1024),
        cost_estimate=pl.CostEstimate(
            flops=2 * rows * tps * mine * cols, bytes_accessed=2 * tps * mine * cols, transcendentals=0
        ),
        name="project_out",
    )(every_head, own_rows, other_rows)


def solution(mesh):
    torus = Mesh(mesh.devices.reshape(16, 4, 4, 2), ("z", "y", "x", "c"))
    sp, tp = ("z", "y"), ("x", "c")
    in_specs = (P(sp, None), P(), P(None, tp), P(), P(), P(tp), P(tp, None))
    return jax.shard_map(
        local, mesh=torus, in_specs=in_specs, out_specs=P(sp, None), check_vma=False
    )
```

```python
import math

import jax
import jax.numpy as jnp
from jax import lax
from jax.experimental import pallas as pl
from jax.experimental.pallas import tpu as pltpu
from jax.sharding import Mesh
from jax.sharding import PartitionSpec as P


HEAD_DIM = 64
TILE = 256
AT_ONCE = 6
VMEM = pltpu.VMEM
SMEM = pltpu.SMEM
HELD = 64 * math.log(2.0)


ROWS_AT_ONCE = 32
NEAR = ((-6, -5, -3, -4), (-2, -1, 1, 0), (5, 4, 2, 3), (9, 8, 6, 7))


def project_kernel(
    hidden_hbm,
    gain_hbm,
    wq_hbm,
    wk_hbm,
    wv_hbm,
    q_ref,
    kv_ref,
    hidden_ref,
    gain_ref,
    wq_ref,
    wkv_ref,
    normed_ref,
    turn_ref,
    sems,
):
    rows, _ = hidden_ref.shape
    mine = 2 * HEAD_DIM
    x = lax.axis_index("x")
    cols = pl.ds(pl.multiple_of((x // 2) * mine, mine), mine)
    pairs = (
        (gain_hbm, gain_ref),
        (hidden_hbm, hidden_ref),
        (wk_hbm.at[:, cols], wkv_ref.at[:, :mine]),
        (wv_hbm.at[:, cols], wkv_ref.at[:, mine:]),
        (wq_hbm, wq_ref),
    )
    copies = [pltpu.make_async_copy(src, dst, sems.at[n]) for n, (src, dst) in enumerate(pairs)]
    for copy in copies:
        copy.start()
    copies[0].wait()
    copies[1].wait()
    for n in range(rows // ROWS_AT_ONCE):
        part = slice(n * ROWS_AT_ONCE, (n + 1) * ROWS_AT_ONCE)
        wide = hidden_ref[part, :].astype(jnp.float32)
        inv = lax.rsqrt(jnp.mean(wide * wide, axis=-1, keepdims=True) + 1e-06)
        normed_ref[part, :] = (wide * inv * gain_ref[...]).astype(jnp.bfloat16)

    copies[2].wait()
    copies[3].wait()
    both = jnp.dot(normed_ref[...], wkv_ref[...], preferred_element_type=jnp.float32)
    k, v = both[:, :mine], both[:, mine:]
    upper = x % 2 == 1
    lane = lax.broadcasted_iota(jnp.int32, k.shape, 1)
    k_side = jnp.where(upper, pltpu.roll(k, HEAD_DIM, 1), k)
    v_side = jnp.where(upper, v, pltpu.roll(v, HEAD_DIM, 1))
    kv = jnp.where(lane < HEAD_DIM, k_side, v_side)
    turn_ref[...] = kv
    few = kv_ref.shape[0] // 2
    for odd in range(2):
        first = turn_ref[pl.ds(odd, few, stride=2), :]
        second = turn_ref[pl.ds(2 * few + odd, few, stride=2), :]
        part = slice(odd * few, (odd + 1) * few)
        kv_ref[part, :] = jnp.where(lax.axis_index("c") == 0, first, second).astype(jnp.bfloat16)

    copies[4].wait()
    q = jnp.dot(normed_ref[...], wq_ref[...], preferred_element_type=jnp.float32)
    q = q.astype(jnp.bfloat16) * jnp.bfloat16(HEAD_DIM**-0.5)
    for dest in range(q_ref.shape[0]):
        q_ref[dest] = q


def attend_kernel(bias_ref, q_ref, kv_ref, out_ref, qs, evens, odds, acc, carry):
    cores, places, half = kv_ref.shape[:3]
    blocks, tok = q_ref.shape[0], q_ref.shape[1]
    mine = 2 * HEAD_DIM
    few, wide = half // 2, TILE // 2
    key_tiles = places * tok // TILE
    tokens = blocks * tok
    row_tiles = tokens // TILE
    lane = lax.broadcasted_iota(jnp.int32, (tok, mine), 1)
    for b in range(blocks):
        q = q_ref[b].astype(jnp.float32)
        qs[b * tok : (b + 1) * tok, :] = jnp.where(lane < HEAD_DIM, q, 0.0).astype(jnp.bfloat16)
        turned = jnp.where(lane < HEAD_DIM, pltpu.roll(q, HEAD_DIM, 1), 0.0)
        qs[tokens + b * tok : tokens + (b + 1) * tok, :] = turned.astype(jnp.bfloat16)
    own = lax.axis_index("y")
    span = len(NEAR)
    for row in range(span):
        for turn in range(span):
            source = lax.rem(span * own + NEAR[row][turn] + places, places)
            place = row * span + lax.rem(own + turn, span)
            for core in range(cores):
                at = pl.multiple_of(place * (tok // 2) + core * few, 16)
                evens[pl.ds(at, few), :] = kv_ref[core, source, :few, :]
                odds[pl.ds(at, few), :] = kv_ref[core, source, few:, :]
    acc[...] = jnp.zeros_like(acc)
    carry[...] = jnp.full(carry.shape, -HELD, jnp.float32)
    from_row = lax.broadcasted_iota(jnp.int32, (TILE, TILE), 0)
    to_col = lax.broadcasted_iota(jnp.int32, (TILE, TILE), 1)
    in_half = (from_row < wide) == (to_col < wide)
    later_pair = ((from_row > to_col) & in_half).astype(jnp.bfloat16)

    def order(lanes):
        return jnp.where(lanes < wide, 2 * lanes, 2 * (lanes - wide) + 1)

    later = (order(from_row) > order(to_col)).astype(jnp.bfloat16)
    rel = lax.axis_index("z") * row_tiles - own * key_tiles

    side = lax.broadcasted_iota(jnp.int32, (2 * mine, mine), 1) // HEAD_DIM
    place = lax.broadcasted_iota(jnp.int32, (2 * mine, mine), 0) // HEAD_DIM
    by_head = (place == side)[:mine].astype(jnp.bfloat16)
    by_key = (place == 2 * side).astype(jnp.bfloat16)

    def largest(rows, groups):
        return jnp.max(jnp.dot(rows * rows, groups, preferred_element_type=jnp.float32))

    key_norm = largest(jnp.concatenate([evens[...], odds[...]], axis=1), by_key)
    query_norm = largest(q_ref[...].reshape(tokens, mine), by_head)
    room = 20.0 - jnp.maximum(bias_ref[0], bias_ref[1])
    tame = (room > 0.0) & (query_norm * key_norm * 1.03 <= room * room)

    def tile(k):
        at = pl.ds(pl.multiple_of(k * wide, wide), wide)
        kv = jnp.concatenate([evens[at, :], odds[at, :]], axis=0)
        raw = lax.dot_general(
            qs[...], kv, (((1,), (1,)), ((), ())), preferred_element_type=jnp.float32
        )
        return kv, jnp.concatenate([raw[:tokens] + bias_ref[0], raw[tokens:] + bias_ref[1]], axis=0)

    def shown(k, z):
        t = lax.broadcasted_iota(jnp.int32, (tokens, TILE), 0)
        s = order(lax.broadcasted_iota(jnp.int32, (tokens, TILE), 1))
        seen = s - t < (rel - k) * TILE
        return jnp.where(jnp.concatenate([seen, seen], axis=0), z, -1e30)

    def step(k, masked):
        kv, z = tile(k)
        if masked:
            z = shown(k, z)
        soft = jnp.maximum(z, jnp.log(1.0 + jnp.exp(jnp.minimum(z, 80.0))))
        between = jnp.dot(soft.astype(jnp.bfloat16), later, preferred_element_type=jnp.float32)
        held = carry[...]
        weight = jnp.exp((z - soft) - between - jnp.concatenate([held, held], axis=1))
        acc[...] += jnp.dot(weight.astype(jnp.bfloat16), kv, preferred_element_type=jnp.float32)
        carry[...] = held + jnp.broadcast_to(between[:, :1] + soft[:, :1], held.shape)

    def tame_step(k, masked):
        kv, z = tile(k)
        if masked:
            z = shown(k, z)
        u = jnp.exp(z)
        u_even, u_odd = u[:, :wide], u[:, wide:]
        even = 1.0 + u_even
        pair = even * (1.0 + u_odd)
        soft = jnp.log(pair)
        short = soft.astype(jnp.bfloat16)
        both = jnp.dot(
            jnp.concatenate([short[:tokens], short[tokens:]], axis=1),
            later_pair,
            preferred_element_type=jnp.float32,
        )
        between = jnp.concatenate([both[:, :wide], both[:, wide:]], axis=0)
        held = carry[...]
        rest = jnp.exp(-(between + held)) / pair
        weight = jnp.concatenate(
            [(u_even * rest).astype(jnp.bfloat16), (u_odd * even * rest).astype(jnp.bfloat16)], axis=1
        )
        acc[...] += jnp.dot(weight, kv, preferred_element_type=jnp.float32)
        carry[...] = held + jnp.broadcast_to(between[:, :1] + soft[:, :1], held.shape)

    crossed = (rel >= 0) & (rel < key_tiles)
    whole = jnp.clip(rel, 0, key_tiles)

    left = lax.rem(whole, AT_ONCE)

    @pl.when(tame & crossed & (left == 0))
    def _():
        for m in range(row_tiles):
            tame_step(rel + row_tiles - 1 - m, True)

    @pl.when(tame & crossed & (left > 0))
    def _():
        for m in range(row_tiles):
            tame_step(rel + row_tiles - 1 - m, True)
        for m in range(row_tiles):
            tame_step(rel - 1 - m, False)

    @pl.when(tame)
    def _():
        start = whole - left

        @pl.loop(0, whole // AT_ONCE)
        def _(n):
            for m in range(AT_ONCE):
                tame_step(start - 1 - AT_ONCE * n - m, False)

    @pl.when(jnp.logical_not(tame))
    def _():
        @pl.loop(0, jnp.where(crossed, row_tiles, 0))
        def _(n):
            step(rel + row_tiles - 1 - n, True)

        @pl.loop(0, whole)
        def _(n):
            step(whole - 1 - n, False)

    mark_row = lax.broadcasted_iota(jnp.int32, (16, mine), 0)
    mark_lane = lax.broadcasted_iota(jnp.int32, (16, mine), 1)
    pick = (mark_row * HEAD_DIM == mark_lane) & (mark_row < 2)
    pick = pick.astype(jnp.bfloat16)
    for n in range(blocks):
        first = slice(n * tok, (n + 1) * tok)
        second = slice(tokens + n * tok, tokens + (n + 1) * tok)
        part = jnp.where(lane < HEAD_DIM, pltpu.roll(acc[first], HEAD_DIM, 1), acc[second]) * 2.0**-64
        decay = jnp.exp(-(jnp.where(lane < HEAD_DIM, carry[first], carry[second]) + HELD))
        out_ref[n, :tok, :] = part.astype(jnp.bfloat16)
        turned = lax.dot_general(
            pick, decay.astype(jnp.bfloat16), (((1,), (1,)), ((), ())), preferred_element_type=jnp.float32
        ).astype(jnp.bfloat16)
        out_ref[n, tok : tok + 16, :] = turned[:, :mine]
        out_ref[n, tok + 16 :, :] = jnp.zeros((16, mine), jnp.bfloat16)
        out_ref[n, tok + 16 :, : tok - mine] = turned[:, mine:]


def combine_kernel(part_ref, out_ref):
    tok, mine = out_ref.shape[1], out_ref.shape[2]
    row = lax.broadcasted_iota(jnp.int32, (16, mine), 0)
    lane = lax.broadcasted_iota(jnp.int32, (16, mine), 1)
    spread = (row == lane // HEAD_DIM).astype(jnp.bfloat16)

    def column(turned):
        return lax.dot_general(
            turned, spread, (((0,), (0,)), ((), ())), preferred_element_type=jnp.float32
        )

    total = part_ref[0, :tok].astype(jnp.float32)
    for n in range(1, part_ref.shape[0]):
        decay = jnp.concatenate(
            [
                column(part_ref[n, tok : tok + 16, :]),
                column(part_ref[n, tok + 16 :, :])[: tok - mine],
            ],
            axis=0,
        )
        total = part_ref[n, :tok].astype(jnp.float32) + decay * total
    attended = total.astype(jnp.bfloat16)
    for dest in range(out_ref.shape[0]):
        out_ref[dest] = attended


def project_out_kernel(heads_ref, own_ref, other_ref, out_ref, joined):
    c = lax.axis_index("c")
    xs, mine = own_ref.shape[0], own_ref.shape[1]
    for side, core in enumerate((c, 1 - c)):
        for x in range(xs):
            col = (side * xs + x) * mine
            joined[:, col : col + mine] = heads_ref[2 * x + core]
    half = xs * mine
    block = 512
    for n in range(out_ref.shape[1] // block):
        cols = slice(n * block, (n + 1) * block)
        total = jnp.dot(
            joined[:, :half], own_ref[:, :, cols].reshape(half, block), preferred_element_type=jnp.float32
        )
        total += jnp.dot(
            joined[:, half:], other_ref[:, :, cols].reshape(half, block), preferred_element_type=jnp.float32
        )
        out_ref[:, cols] = total.astype(jnp.bfloat16)


def local(hidden, norm_gain, query_weight, key_weight, value_weight, head_bias, output_weight):
    rows, width = hidden.shape
    zs, ys, xs = lax.axis_size("z"), lax.axis_size("y"), lax.axis_size("x")
    cores = lax.axis_size("c")
    tps = xs * cores
    mine = 2 * HEAD_DIM
    vmem = pl.BlockSpec(memory_space=VMEM)
    smem = pl.BlockSpec(memory_space=SMEM)
    anywhere = pl.BlockSpec(memory_space=pl.ANY)

    queries, kv = pl.pallas_call(
        project_kernel,
        in_specs=[anywhere] * 5,
        out_specs=[vmem, vmem],
        out_shape=[
            jax.ShapeDtypeStruct((ys, rows, mine), jnp.bfloat16),
            jax.ShapeDtypeStruct((rows // cores, mine), jnp.bfloat16),
        ],
        scratch_shapes=[
            VMEM((rows, width), jnp.bfloat16),
            VMEM((1, width), jnp.float32),
            VMEM((width, mine), jnp.bfloat16),
            VMEM((width, 2 * mine), jnp.bfloat16),
            VMEM((rows, width), jnp.bfloat16),
            VMEM((rows, mine), jnp.float32),
            pltpu.SemaphoreType.DMA((5,)),
        ],
        compiler_params=pltpu.CompilerParams(vmem_limit_bytes=56 * 1024 * 1024),
        cost_estimate=pl.CostEstimate(
            flops=2 * rows * width * 3 * mine,
            bytes_accessed=2 * width * (rows + 3 * mine),
            transcendentals=0,
        ),
        name="project",
    )(hidden, norm_gain[None, :], query_weight, key_weight, value_weight)

    pairs = []
    for z in range(zs):
        for y in range(ys):
            super_row, row = divmod(z, ys)
            near = (ys * super_row + NEAR[row][(y - super_row) % ys]) % zs
            pairs.append((z * ys + y, near * ys + super_row))
    moved = lax.ppermute(kv, ("z", "y"), pairs)
    row_q = lax.all_to_all(queries, "y", 0, 0, tiled=True)
    fan = jnp.broadcast_to(output_weight[None], (xs, *output_weight.shape))
    row_q, moved, fan = lax.optimization_barrier((row_q, moved, fan))
    own_rows = lax.all_to_all(fan, "x", 0, 0, tiled=True)
    quarter_half = lax.all_gather(moved, "z", axis=0)
    quarter = lax.all_gather(quarter_half, "c", axis=0)
    quarter, own_rows = lax.optimization_barrier((quarter, own_rows))
    other_rows = lax.ppermute(own_rows, "c", [(0, 1), (1, 0)])

    tokens = ys * rows
    part = pl.pallas_call(
        attend_kernel,
        in_specs=[smem, vmem, vmem],
        out_specs=vmem,
        out_shape=jax.ShapeDtypeStruct((ys, rows + 32, mine), jnp.bfloat16),
        scratch_shapes=[
            VMEM((2 * tokens, mine), jnp.bfloat16),
            VMEM((zs * rows // 2, mine), jnp.bfloat16),
            VMEM((zs * rows // 2, mine), jnp.bfloat16),
            VMEM((2 * tokens, mine), jnp.float32),
            VMEM((2 * tokens, mine), jnp.float32),
        ],
        compiler_params=pltpu.CompilerParams(vmem_limit_bytes=24 * 1024 * 1024),
        cost_estimate=pl.CostEstimate(flops=10**10, bytes_accessed=2 * 10**6, transcendentals=0),
        name="attend",
    )(head_bias, row_q, quarter)

    parts = lax.all_to_all(part, "y", 0, 0, tiled=True)
    attended = pl.pallas_call(
        combine_kernel,
        in_specs=[vmem],
        out_specs=vmem,
        out_shape=jax.ShapeDtypeStruct((tps, rows, mine), jnp.bfloat16),
        compiler_params=pltpu.CompilerParams(vmem_limit_bytes=16 * 1024 * 1024),
        name="combine",
    )(parts)
    every_head = lax.all_to_all(attended, ("x", "c"), 0, 0, tiled=True)
    cols = output_weight.shape[1]
    return pl.pallas_call(
        project_out_kernel,
        in_specs=[vmem, vmem, vmem],
        out_specs=vmem,
        out_shape=jax.ShapeDtypeStruct((rows, cols), jnp.bfloat16),
        scratch_shapes=[VMEM((rows, tps * mine), jnp.bfloat16)],
        compiler_params=pltpu.CompilerParams(vmem_limit_bytes=20 * 1024 * 1024),
        cost_estimate=pl.CostEstimate(
            flops=2 * rows * tps * mine * cols, bytes_accessed=2 * tps * mine * cols, transcendentals=0
        ),
        name="project_out",
    )(every_head, own_rows, other_rows)


def solution(mesh):
    torus = Mesh(mesh.devices.reshape(16, 4, 4, 2), ("z", "y", "x", "c"))
    sp, tp = ("z", "y"), ("x", "c")
    in_specs = (P(sp, None), P(), P(None, tp), P(), P(), P(tp), P(tp, None))
    return jax.shard_map(
        local, mesh=torus, in_specs=in_specs, out_specs=P(sp, None), check_vma=False
    )
```
